256 devices in a mesh: kv: 32 (over z, x), tp: 8 (over y, core).
Axes of the slice: x: 4, y: 4, z: 8, core: 2. Of those that a mesh axis runs over, the one named last changes fastest.
Arguments:
- tokens: bfloat16 [16384, 2048], P('kv'), may hold values from -64 to 64
- query_weight: bfloat16 [2048, 2048], P(None, 'tp'), may hold values from -0.1875 to 0.1875
- chosen_key_weight: bfloat16 [2048, 512], P(None, 'tp'), may hold values from -0.125 to 0.125
- chosen_value_weight: bfloat16 [2048, 512], P(None, 'tp'), may hold values from -0.125 to 0.125
- summary_key_weight: bfloat16 [2048, 512], P(None, 'tp'), may hold values from -0.125 to 0.125
- summary_value_weight: bfloat16 [2048, 512], P(None, 'tp'), may hold values from -0.125 to 0.125
- squeeze_key_in: bfloat16 [2048, 128], replicated, may hold values from -0.125 to 0.125
- squeeze_key_out: bfloat16 [128, 64], replicated, may hold values from -1 to 1
- squeeze_value_in: bfloat16 [2048, 128], replicated, may hold values from -0.125 to 0.125
- squeeze_value_out: bfloat16 [128, 64], replicated, may hold values from -2 to 2
- gate_weight: bfloat16 [2, 2048, 32], P(None, None, 'tp'), may hold values from -0.125 to 0.125
- output_weight: bfloat16 [2048, 2048], P('tp'), may hold values from -1 to 1
- chosen_blocks: int32 [8, 512, 16], P('tp', 'kv'), may hold values from 0 to 511, as said below
Outputs:
- attended: bfloat16 [16384, 2048], P(('kv', 'tp'))
The draws below stay inside these ranges and needn't reach their ends.
Inputs may be any that keep to these rules, and one draw needn't show every extreme that they name: `chosen_blocks`: each row lists 16 different blocks. The row of query block b lists b, lists b - 1 where b > 0, and lists block 0. Take the blocks at or below their query block that the rows of the query blocks of one index of kv list for one key head: at most 4 different ones lie among the positions of any other single index of kv, and exactly 4 among the positions of the first index, for every index after the first.
All inputs are finite; a program needn't handle non-finite values.
Results may differ from the reference program's by a relative error of at most 0.03.
Values may be sent and summed in bfloat16 or wider, within the bound.
No kernel may reach another device: no remote copies, remote signals or barrier semaphores. Data moves between devices by JAX's collectives and lax.ppermute only.
A program may use at most 128 MiB of HBM per device.

```python
import jax
import jax.numpy as jnp
from jax import lax

D = 2048
H = 32
KVH = 8
HD = 64
CMP_LEN = 32
CMP_STRIDE = 16
CMP_HIDDEN = 128
BLK = 32
NSEL = 16
CAP = 4
TOK_DEV = 512
SEQ = 16384
NB = 512
N_TP = 8


def draw_tokens(key, part):
    first, second, third = jax.random.split(key, 3)
    base = jax.random.truncated_normal(first, -4.0, 4.0, (SEQ, D), jnp.float32)
    return base.astype(jnp.bfloat16)


def draw_chosen_blocks(key, part):
    per_dev = TOK_DEV // BLK
    blocks = SEQ // BLK
    owners = blocks // per_dev
    first, second = jax.random.split(jax.random.fold_in(key, 7))
    inner = jnp.arange(per_dev, dtype=jnp.int32)
    pick = jax.random.randint(first, (KVH, owners, owners, per_dev), 0, 1 << 20) * per_dev + inner
    asker = jnp.arange(owners, dtype=jnp.int32)[:, None, None]
    holder = jnp.arange(owners, dtype=jnp.int32)[None, :, None]
    inner_row = inner[None, None, :]
    pinned = (holder == 0) & (inner_row == 0) | (holder == asker - 1) & (inner_row == per_dev - 1)
    pinned = pinned | (holder == asker - owners // 2) & (inner_row == 1)
    pick = pick + pinned.astype(jnp.int32) * (1 << 28)
    above = jnp.sum((pick[..., None, :] > pick[..., :, None]).astype(jnp.int32), -1)
    subset = above < CAP
    query_block = jnp.arange(blocks, dtype=jnp.int32)[:, None]
    key_block = jnp.arange(blocks, dtype=jnp.int32)[None, :]
    asking = query_block // per_dev
    holding = key_block // per_dev
    granted = subset[:, query_block[:, 0] // per_dev].reshape(KVH, blocks, blocks)
    past = key_block <= query_block
    usable = past & ((holding == asking) | (holding < asking) & granted)
    forced = (key_block == query_block) | (key_block == query_block - 1) | (key_block == 0)
    forced = forced | (query_block % per_dev == 0) & (asking >= owners // 2) & (key_block == (asking - owners // 2) * per_dev + 1)
    forced = forced | (query_block % per_dev == per_dev - 1) & (asking >= 1) & (holding == 0) & granted
    forced = forced & usable
    tier = jnp.where(forced, 3, jnp.where(usable, 2, jnp.where(past, 0, 1)))
    noise = jax.random.randint(second, (KVH, blocks, blocks), 0, 4096) // (1 + holding)
    score = tier * (1 << 24) + noise * blocks + key_block
    return lax.top_k(score, NSEL)[1].astype(jnp.int32)


def block_scale(stream_key, extent, cuts, low, high):
    level, own = 1.0, jax.random.fold_in(stream_key, 6)
    for position, shards_of in cuts:
        draws = jnp.exp(jax.random.uniform(jax.random.fold_in(own, position), (shards_of,), jnp.float32, low / len(cuts), high / len(cuts)))
        level = level * jnp.repeat(draws, extent[position] // shards_of).reshape([-1 if axis == position else 1 for axis in range(len(extent))])
    return level


def bell_draw(rng, shape, spread, limit, pieces=(), kind=jnp.bfloat16):
    factor_of = block_scale(rng, shape, pieces, -0.22, 0.18) if pieces else 1.0
    array = jax.random.normal(rng, shape, jnp.float32) * spread * factor_of
    return jnp.minimum(jnp.maximum(array, -limit), limit).astype(kind)


def setup_inputs(seed: int = 0) -> dict:
    seeds = jax.random.split(jax.random.key(seed), 14)
    tokens = draw_tokens(jax.random.fold_in(seeds[13], 71), 0)
    query_weight = bell_draw(seeds[1], (D, H * HD), (D * 4 // 9) ** -0.5, 0.1875, ((1, 8),))
    chosen_key_weight = bell_draw(seeds[2], (D, KVH * HD), D ** -0.5, 0.125, ((1, 8),))
    chosen_value_weight = bell_draw(seeds[3], (D, KVH * HD), D ** -0.5, 0.125, ((1, 8),))
    summary_key_weight = bell_draw(seeds[4], (D, KVH * HD), D ** -0.5, 0.125, ((1, 8),))
    summary_value_weight = bell_draw(seeds[5], (D, KVH * HD), D ** -0.5, 0.125, ((1, 8),))
    squeeze_key_in = bell_draw(seeds[6], (CMP_LEN * HD, CMP_HIDDEN), (CMP_LEN * HD) ** -0.5, 0.125)
    squeeze_key_out = bell_draw(seeds[7], (CMP_HIDDEN, HD), (CMP_HIDDEN // 4) ** -0.5, 1.0)
    squeeze_value_in = bell_draw(seeds[8], (CMP_LEN * HD, CMP_HIDDEN), (CMP_LEN * HD) ** -0.5, 0.125)
    squeeze_value_out = bell_draw(seeds[9], (CMP_HIDDEN, HD), (CMP_HIDDEN // 16) ** -0.5, 2.0)
    gate_weight = bell_draw(seeds[10], (2, D, H), D ** -0.5, 0.125, ((2, 8),))
    output_weight = bell_draw(seeds[11], (H * HD, D), (H * HD // 64) ** -0.5, 1.0, ((0, 8),))
    chosen_blocks = draw_chosen_blocks(jax.random.fold_in(seeds[13], 71), 0)
    return dict(tokens=tokens, query_weight=query_weight, chosen_key_weight=chosen_key_weight, chosen_value_weight=chosen_value_weight, summary_key_weight=summary_key_weight, summary_value_weight=summary_value_weight, squeeze_key_in=squeeze_key_in, squeeze_key_out=squeeze_key_out, squeeze_value_in=squeeze_value_in, squeeze_value_out=squeeze_value_out, gate_weight=gate_weight, output_weight=output_weight, chosen_blocks=chosen_blocks)


ROTARY_BASE = 10000.0
NEGATIVE_FILL = -1e30


def rotate(values, positions):
    halfway = values.shape[-1] // 2
    inverse = ROTARY_BASE ** (-jnp.arange(halfway, dtype=jnp.float32) / halfway)
    angles = positions.astype(jnp.float32)[:, None] * inverse[None, :]
    cosine_rows = jnp.cos(angles)[:, None, :]
    sine_rows = jnp.sin(angles)[:, None, :]
    former = values[..., :halfway]
    latter = values[..., halfway:]
    return jnp.concatenate([former * cosine_rows - latter * sine_rows, latter * cosine_rows + former * sine_rows], -1)


def squeeze_windows(raw_rows, weight_in, weight_out):
    length = raw_rows.shape[0]
    head_count = raw_rows.shape[1]
    head_width = raw_rows.shape[2]
    padded = jnp.concatenate([raw_rows, jnp.zeros((CMP_STRIDE, head_count, head_width), raw_rows.dtype)], 0)
    segments = padded.reshape(length // CMP_STRIDE + 1, CMP_STRIDE, head_count, head_width)
    windows = jnp.concatenate([segments[:-1], segments[1:]], 1)
    flattened = windows.transpose(0, 2, 1, 3).reshape(-1, CMP_LEN * head_width)
    hidden = jax.nn.gelu(jnp.dot(flattened, weight_in, preferred_element_type=jnp.float32)).astype(jnp.bfloat16)
    return jnp.dot(hidden, weight_out, preferred_element_type=jnp.float32).reshape(length // CMP_STRIDE, head_count, head_width)


def widen(values):
    return lax.optimization_barrier(values.astype(jnp.bfloat16)).astype(jnp.float32)


def softmax_mix(scores, visible, values, pattern):
    largest = jnp.max(jnp.where(visible, scores, NEGATIVE_FILL), -1, keepdims=True)
    weights = jnp.where(visible, jnp.exp(scores - largest), 0.0)
    summed = jnp.sum(weights, -1)[..., None]
    return jnp.einsum(pattern, widen(weights), values) / jnp.maximum(summed, 1.0)


def reference(tokens, query_weight, chosen_key_weight, chosen_value_weight, summary_key_weight, summary_value_weight,
              squeeze_key_in, squeeze_key_out, squeeze_value_in, squeeze_value_out, gate_weight, output_weight, chosen_blocks):
    positions = jnp.arange(SEQ, dtype=jnp.int32)
    per_group = H // KVH
    queries = widen(rotate(jnp.dot(tokens, query_weight, preferred_element_type=jnp.float32).reshape(SEQ, H, HD), positions))
    queries = queries.reshape(SEQ, KVH, per_group, HD)
    chosen_keys = widen(rotate(jnp.dot(tokens, chosen_key_weight, preferred_element_type=jnp.float32).reshape(SEQ, KVH, HD), positions))
    chosen_values = widen(jnp.dot(tokens, chosen_value_weight, preferred_element_type=jnp.float32)).reshape(SEQ, KVH, HD)
    raw_keys = jnp.dot(tokens, summary_key_weight, preferred_element_type=jnp.float32).astype(jnp.bfloat16).reshape(SEQ, KVH, HD)
    raw_values = jnp.dot(tokens, summary_value_weight, preferred_element_type=jnp.float32).astype(jnp.bfloat16).reshape(SEQ, KVH, HD)
    summary_count = SEQ // CMP_STRIDE
    summary_ends = jnp.arange(summary_count, dtype=jnp.int32) * CMP_STRIDE + CMP_LEN - 1
    summary_keys = widen(rotate(squeeze_windows(raw_keys, squeeze_key_in, squeeze_key_out), summary_ends))
    summary_values = widen(squeeze_windows(raw_values, squeeze_value_in, squeeze_value_out))
    block_keys = chosen_keys.reshape(NB, BLK, KVH, HD).transpose(2, 0, 1, 3)
    block_values = chosen_values.reshape(NB, BLK, KVH, HD).transpose(2, 0, 1, 3)
    first_gates = jax.nn.sigmoid(jnp.dot(tokens, gate_weight[0], preferred_element_type=jnp.float32))
    second_gates = jax.nn.sigmoid(jnp.dot(tokens, gate_weight[1], preferred_element_type=jnp.float32))
    scaling = HD ** -0.5
    group_ids = jnp.arange(KVH, dtype=jnp.int32)[:, None]

    def one_block(block_id):
        first_row = block_id * BLK
        rows_here = first_row + jnp.arange(BLK, dtype=jnp.int32)
        block_queries = lax.dynamic_slice_in_dim(queries, first_row, BLK, 0)
        scores = jnp.einsum('qgrd,ngd->grqn', block_queries, summary_keys) * scaling
        visible = (summary_ends[None, :] <= rows_here[:, None])[None, None]
        compressed = softmax_mix(scores, visible, summary_values, 'grqn,ngd->grqd')
        listed = lax.dynamic_index_in_dim(chosen_blocks, block_id, 1, keepdims=False)
        picked_keys = block_keys[group_ids, listed]
        picked_values = block_values[group_ids, listed].reshape(KVH, NSEL * BLK, HD)
        scores = jnp.einsum('qgrd,gkld->grqkl', block_queries, picked_keys).reshape(KVH, per_group, BLK, NSEL * BLK) * scaling
        key_positions = (listed[:, :, None] * BLK + jnp.arange(BLK, dtype=jnp.int32)).reshape(KVH, NSEL * BLK)
        visible = (key_positions[:, None, :] <= rows_here[None, :, None])[:, None]
        selected = softmax_mix(scores, visible, picked_values, 'grqk,gkd->grqd')
        gate_one = lax.dynamic_slice_in_dim(first_gates, first_row, BLK, 0).reshape(BLK, KVH, per_group).transpose(1, 2, 0)[..., None]
        gate_two = lax.dynamic_slice_in_dim(second_gates, first_row, BLK, 0).reshape(BLK, KVH, per_group).transpose(1, 2, 0)[..., None]
        blended = gate_one * compressed + gate_two * selected
        return blended.transpose(2, 0, 1, 3).reshape(BLK, H * HD).astype(jnp.bfloat16)

    blended = lax.map(one_block, jnp.arange(NB, dtype=jnp.int32)).reshape(SEQ, H * HD)
    heads_per_device = H // N_TP
    grouped_rows = blended.reshape(SEQ, N_TP, heads_per_device * HD)
    grouped_weight = output_weight.reshape(N_TP, heads_per_device * HD, D)

    def add_group(summed, group_id):
        rows_part = lax.dynamic_index_in_dim(grouped_rows, group_id, 1, keepdims=False)
        weight_part = lax.dynamic_index_in_dim(grouped_weight, group_id, 0, keepdims=False)
        part_sum = widen(jnp.dot(rows_part, weight_part, preferred_element_type=jnp.float32))
        return summed + part_sum, None

    grand_total, _ = lax.scan(add_group, jnp.zeros((SEQ, D), jnp.float32), jnp.arange(N_TP, dtype=jnp.int32))
    return grand_total.astype(jnp.bfloat16)
```

```python
import jax
import jax.numpy as jnp
import numpy as np
from jax import lax
from jax.experimental import pallas as pl
from jax.experimental.pallas import tpu as pltpu
from jax.sharding import PartitionSpec as P

HD = 64
CMP_STRIDE = 16
BLK = 32
NSEL = 16
CAP = 4
ROTARY_BASE = 10000.0
NEG = -1e30
FLOOR = -1e29
TOK = 512
PEERS = 32
NSUM = 32
ROWS = 40
QB = TOK // BLK
HEADS = 4
NBLK = PEERS * QB
UNUSED = 99.0

INVERSE = (ROTARY_BASE ** (-np.arange(HD // 2, dtype=np.float64) / (HD // 2))).astype(np.float32)
INVERSE_ROW = np.tile(INVERSE, 4)[None, :]
SIGN_ROW = np.tile(np.repeat(np.array([-1.0, 1.0], np.float32), HD // 2), 2)[None, :]

bf16 = jnp.bfloat16
f32 = jnp.float32


def dot(a, b):
    return jnp.dot(a, b, preferred_element_type=f32)


def lanes_of(shape):
    return lax.broadcasted_iota(jnp.int32, shape, len(shape) - 1)


def rows_of(shape):
    return lax.broadcasted_iota(jnp.int32, shape, len(shape) - 2)


def turned(x, cosine, sine):
    lane = lanes_of(x.shape)
    swapped = jnp.where(lane % HD < HD // 2, pltpu.roll(x, 128 - HD // 2, 1), pltpu.roll(x, HD // 2, 1))
    return x * cosine + swapped * sine


def gelu(x):
    return 0.5 * x * (1.0 + jnp.tanh(np.float32(np.sqrt(2.0 / np.pi)) * (x + 0.044715 * (x * x * x))))


def squeeze_out(pre_k, pre_v, out_k, out_v, cosine, sine):
    hidden = jnp.concatenate([gelu(pre_k).astype(bf16), gelu(pre_v).astype(bf16)], 1)
    zero = jnp.zeros(out_k.shape, bf16)
    weight = jnp.concatenate(
        [jnp.concatenate([out_k, zero], 1), jnp.concatenate([zero, out_v], 1)], 0
    )
    both = dot(hidden, weight)
    return jnp.where(lanes_of(both.shape) < HD, turned(both, cosine, sine), both)


def summary_kernel(
    rank_ref, tokens_ref, wk_ref, wv_ref, ink_ref, inv_ref, outk_ref, outv_ref, cos_ref, sin_ref,
    chosen_ref, payload_ref, code_ref, raw_ref,
):
    rank = rank_ref[0]
    weight = jnp.concatenate([wk_ref[...], wv_ref[...]], 1)
    raw_ref[...] = dot(tokens_ref[...], weight).astype(bf16).astype(f32)
    zero = jnp.zeros((HD, 128), bf16)
    total = jnp.zeros((NSUM, 512), f32)
    for p in range(0, CMP_STRIDE, 2):
        left = []
        right = []
        for q in (p, p + 1):
            left.append(raw_ref[pl.ds(q, NSUM, stride=CMP_STRIDE), :].astype(bf16))
            low = pl.ds(q * HD, HD)
            high = pl.ds((q + CMP_STRIDE) * HD, HD)
            right.append(jnp.concatenate([ink_ref[low, :], ink_ref[high, :], zero, zero], 1))
            right.append(jnp.concatenate([zero, zero, inv_ref[low, :], inv_ref[high, :]], 1))
        total = total + dot(jnp.concatenate(left, 1), jnp.concatenate(right, 0))
    low_k, high_k = total[:, :128], total[:, 128:256]
    low_v, high_v = total[:, 256:384], total[:, 384:]
    pre_k = low_k + pltpu.roll(high_k, NSUM - 1, 0)
    pre_v = low_v + pltpu.roll(high_v, NSUM - 1, 0)
    summaries = squeeze_out(
        pre_k, pre_v, outk_ref[...], outv_ref[...], cos_ref[...], sin_ref[...]
    )
    chosen = chosen_ref[...]
    query_block = rank * QB + rows_of(chosen.shape)
    wanted = jnp.where((chosen <= query_block) & (chosen // QB != rank), chosen, -1)
    every = lanes_of((QB, NBLK))
    hit = jnp.zeros((QB, NBLK), f32)
    for k in range(NSEL):
        hit = jnp.where(every == wanted[:, k : k + 1], 1.0, hit)
    present = jnp.broadcast_to(jnp.max(hit, 0, keepdims=True), (8, NBLK))
    lane = lanes_of((8, NBLK))
    running = present
    for step in (1, 2, 4, 8):
        running = running + jnp.where(lane % QB >= step, pltpu.roll(running, step, 1), 0.0)
    code = jnp.where(present > 0.0, running - present, UNUSED)
    code_ref[...] = code
    payload = jnp.concatenate(
        [
            summaries,
            low_k[NSUM - 1 :], low_v[NSUM - 1 :], high_k[:1], high_v[:1],
            code[:1, :128], code[:1, 128:256], code[:1, 256:384], code[:1, 384:],
        ],
        0,
    ).astype(bf16)
    for peer in range(PEERS):
        payload_ref[peer] = payload


def project_kernel(
    rank_ref, tokens_ref, wq_ref, wk_ref, wv_ref, gate_ref, cos_ref, sin_ref, chosen_ref, code_ref,
    query_ref, pair_ref, gates_ref, place_ref, bound_ref,
):
    rank = rank_ref[0]
    tokens = tokens_ref[...]
    cosine = cos_ref[...]
    sine = sin_ref[...]
    lane = lanes_of((TOK, 128))
    queries = dot(tokens, wq_ref[...]) * np.float32(HD ** -0.5)
    for pair in range(2):
        both = turned(queries[:, 128 * pair : 128 * pair + 128], cosine, sine)
        for half in range(2):
            head = 2 * pair + half
            one = both if half == 0 else pltpu.roll(both, HD, 1)
            one = jnp.where(lane < HD, one, 0.0).astype(bf16)
            for b in range(QB):
                query_ref[b, head * BLK : (head + 1) * BLK, :] = one[b * BLK : (b + 1) * BLK]
    weight = jnp.concatenate([wk_ref[...], wv_ref[...]], 1)
    both = dot(tokens, weight)
    pair_ref[...] = jnp.where(lane < HD, turned(both, cosine, sine), both).astype(bf16)
    weight = jnp.concatenate([gate_ref[0], gate_ref[1]], 1)
    gates_ref[...] = jax.nn.sigmoid(dot(tokens, weight))
    chosen = chosen_ref[...]
    query_block = rank * QB + rows_of(chosen.shape)
    code = code_ref[...]
    code = jnp.concatenate([code, code], 0)
    every = lanes_of((QB, NBLK))
    slot_lane = lanes_of((QB, NSEL))
    slot = jnp.zeros((QB, NSEL), f32)
    for k in range(NSEL):
        found = jnp.where(every == chosen[:, k : k + 1], code, 0.0)
        slot = jnp.where(slot_lane == k, jnp.sum(found, 1, keepdims=True), slot)
    holder = chosen // QB
    place = jnp.where(
        holder == rank, PEERS * CAP + chosen % QB, holder * CAP + slot.astype(jnp.int32)
    )
    place_ref[...] = jnp.where(chosen <= query_block, place, PEERS * CAP)
    order = jnp.where(chosen < query_block, -1.0, jnp.where(chosen > query_block, 1.0, 0.0))
    spread = (lanes_of((NSEL, NSEL * BLK)) // BLK == rows_of((NSEL, NSEL * BLK))).astype(bf16)
    inner = (lanes_of((QB, NSEL * BLK)) % BLK).astype(f32)
    bound_ref[...] = dot(order.astype(bf16), spread) * 64.0 + inner


def pick_kernel(rank_ref, arrived_ref, pair_ref, picked_ref, ids_ref, ids_smem, sem):
    rank = rank_ref[0]
    flat = arrived_ref[...].reshape(PEERS * ROWS, 128)
    shape = (PEERS, PEERS * ROWS)
    chosen_row = (lanes_of(shape) == rows_of(shape) * ROWS + NSUM + 4 + rank // 8).astype(bf16)
    codes = dot(chosen_row, flat)
    lane = lanes_of((PEERS, 128))
    mine = lane // QB == rank % 8
    inner = (lane % QB).astype(f32)
    ids = jnp.zeros((PEERS, 128), f32)
    for s in range(CAP):
        value = jnp.sum(jnp.where(mine & (codes == float(s)), inner, 0.0), 1, keepdims=True)
        ids = jnp.where(lane == s, value, ids)
    ids_ref[...] = ids.astype(jnp.int32)
    copy = pltpu.make_async_copy(ids_ref, ids_smem, sem)
    copy.start()
    copy.wait()

    def one_peer(peer, carry):
        for s in range(CAP):
            start = pl.multiple_of(ids_smem[peer, s] * BLK, BLK)
            picked_ref[peer, s * BLK : (s + 1) * BLK, :] = pair_ref[pl.ds(start, BLK), :]
        return carry

    lax.fori_loop(0, PEERS, one_peer, 0)


def mixed_heads(result, gates, first):
    lane = lanes_of((BLK, 128))
    halves = []
    for pair in range(2):
        gated = []
        for head in (2 * pair, 2 * pair + 1):
            gate = gates[:, first + head : first + head + 1]
            gated.append(result[head * BLK : (head + 1) * BLK] * gate)
        halves.append(jnp.where(lane < HD, pltpu.roll(gated[0], HD, 1), gated[1]))
    return halves


def compressed_kernel(
    rank_ref, arrived_ref, query_ref, gates_ref, outk_ref, outv_ref, cos_ref, sin_ref,
    mixed_ref, key_ref, value_ref,
):
    rank = rank_ref[0]
    flat = arrived_ref[...].reshape(PEERS * ROWS, 128)
    shape = (4 * PEERS, PEERS * ROWS)
    row = rows_of(shape)
    kind = row // PEERS
    source = row % PEERS + kind % 2
    target = source * ROWS + NSUM + jnp.where(kind == 0, 0, jnp.where(kind == 1, 2, jnp.where(kind == 2, 1, 3)))
    edges = dot(((lanes_of(shape) == target) & (source < PEERS)).astype(bf16), flat)
    pre_k = edges[:PEERS] + edges[PEERS : 2 * PEERS]
    pre_v = edges[2 * PEERS : 3 * PEERS] + edges[3 * PEERS :]
    last = squeeze_out(pre_k, pre_v, outk_ref[...], outv_ref[...], cos_ref[...], sin_ref[...])
    is_last = rows_of((NSUM, 128)) == NSUM - 1
    lane = lanes_of((NSUM, 128))
    for peer in range(PEERS):
        chunk = arrived_ref[peer, :NSUM, :].astype(f32)
        chunk = jnp.where(is_last, last[peer : peer + 1], chunk)
        value_ref[peer * NSUM : (peer + 1) * NSUM, :] = jnp.where(lane < HD, 1.0, chunk).astype(bf16)
        key_ref[peer * NSUM : (peer + 1) * NSUM, :] = chunk.astype(bf16)
    columns = lanes_of((HEADS * BLK, PEERS * NSUM))
    inside = lax.broadcasted_iota(jnp.int32, (HEADS * BLK, 1), 0) % BLK

    def one_block(b, carry):
        scores = lax.dot_general(
            query_ref[b], key_ref[...], (((1,), (1,)), ((), ())), preferred_element_type=f32
        )
        limit = (rank * TOK + b * BLK + inside - (2 * CMP_STRIDE - 1)) >> 4
        scores = jnp.where(columns <= limit, scores, NEG)
        largest = jnp.maximum(jnp.max(scores, 1, keepdims=True), FLOOR)
        weights = jnp.exp(scores - largest).astype(bf16)
        result = dot(weights, value_ref[...])
        result = result / jnp.maximum(pltpu.roll(result, HD, 1), 1.0)
        start = pl.multiple_of(b * BLK, BLK)
        halves = mixed_heads(result, gates_ref[pl.ds(start, BLK), :], 0)
        mixed_ref[pl.ds(start, BLK), :128] = halves[0]
        mixed_ref[pl.ds(start, BLK), 128:] = halves[1]
        return carry

    lax.fori_loop(0, QB, one_block, 0)


def selected_kernel(
    place_ref, fetched_ref, pair_ref, query_ref, gates_ref, mixed_ref, bound_ref,
    out_ref, stock_ref, key_ref, sems,
):
    copies = [
        pltpu.make_async_copy(fetched_ref, stock_ref.at[pl.ds(0, PEERS * CAP * BLK)], sems.at[0]),
        pltpu.make_async_copy(pair_ref, stock_ref.at[pl.ds(PEERS * CAP * BLK, TOK)], sems.at[1]),
    ]
    for copy in copies:
        copy.start()
    for copy in copies:
        copy.wait()
    inside = (lax.broadcasted_iota(jnp.int32, (HEADS * BLK, 1), 0) % BLK).astype(f32)
    lane = lanes_of((NSEL * BLK, 128))

    def one_block(b, carry):
        for k in range(NSEL):
            start = pl.multiple_of(place_ref[b, k] * BLK, BLK)
            key_ref[k * BLK : (k + 1) * BLK, :] = stock_ref[pl.ds(start, BLK), :]
        keys = key_ref[...]
        scores = lax.dot_general(
            query_ref[b], keys, (((1,), (1,)), ((), ())), preferred_element_type=f32
        )
        scores = jnp.where(bound_ref[pl.ds(b, 1), :] <= inside, scores, NEG)
        largest = jnp.max(scores, 1, keepdims=True)
        weights = jnp.exp(scores - largest).astype(bf16)
        values = jnp.where(lane < HD, jnp.ones_like(keys), keys)
        result = dot(weights, values)
        result = result / pltpu.roll(result, HD, 1)
        start = pl.multiple_of(b * BLK, BLK)
        halves = mixed_heads(result, gates_ref[pl.ds(start, BLK), :], HEADS)
        out_ref[pl.ds(start, BLK), :128] = (mixed_ref[pl.ds(start, BLK), :128] + halves[0]).astype(bf16)
        out_ref[pl.ds(start, BLK), 128:] = (mixed_ref[pl.ds(start, BLK), 128:] + halves[1]).astype(bf16)
        return carry

    lax.fori_loop(0, QB, one_block, 0)


VMEM = pl.BlockSpec(memory_space=pltpu.VMEM)
SMEM = pl.BlockSpec(memory_space=pltpu.SMEM)
ANY = pl.BlockSpec(memory_space=pl.ANY)


def shape_of(shape, dtype):
    return jax.ShapeDtypeStruct(shape, dtype)


def tables(positions):
    angles = positions.astype(f32)[:, None] * jnp.asarray(INVERSE_ROW)
    return jnp.cos(angles), jnp.sin(angles) * jnp.asarray(SIGN_ROW)


def on_device(
    tokens, query_weight, chosen_key_weight, chosen_value_weight, summary_key_weight,
    summary_value_weight, squeeze_key_in, squeeze_key_out, squeeze_value_in, squeeze_value_out,
    gate_weight, output_weight, chosen_blocks,
):
    kv_rank = lax.axis_index("kv")
    rank = kv_rank.reshape(1).astype(jnp.int32)
    chosen = chosen_blocks[0]
    ends = (kv_rank * NSUM + jnp.arange(NSUM, dtype=jnp.int32)) * CMP_STRIDE + 2 * CMP_STRIDE - 1
    end_cos, end_sin = tables(ends)
    payload, code = pl.pallas_call(
        summary_kernel,
        name="summaries",
        out_shape=(shape_of((PEERS, ROWS, 128), bf16), shape_of((8, NBLK), f32)),
        in_specs=[SMEM] + [VMEM] * 10,
        out_specs=(VMEM, VMEM),
        scratch_shapes=[pltpu.VMEM((TOK, 128), f32)],
        cost_estimate=pl.CostEstimate(flops=10**9, bytes_accessed=5 * 10**6, transcendentals=0),
    )(
        rank, tokens, summary_key_weight, summary_value_weight, squeeze_key_in, squeeze_value_in,
        squeeze_key_out, squeeze_value_out, end_cos, end_sin, chosen,
    )
    arrived = lax.all_to_all(payload, "kv", 0, 0, tiled=True)
    cosine, sine = tables(kv_rank * TOK + jnp.arange(TOK, dtype=jnp.int32))
    queries, pairs, gates, place, bound = pl.pallas_call(
        project_kernel,
        name="projections",
        out_shape=(
            shape_of((QB, HEADS * BLK, 128), bf16),
            shape_of((TOK, 128), bf16),
            shape_of((TOK, 2 * HEADS), f32),
            shape_of((QB, NSEL), jnp.int32),
            shape_of((QB, NSEL * BLK), f32),
        ),
        in_specs=[SMEM] + [VMEM] * 9,
        out_specs=(VMEM,) * 5,
        cost_estimate=pl.CostEstimate(flops=10**10, bytes_accessed=5 * 10**6, transcendentals=0),
    )(
        rank, tokens, query_weight, chosen_key_weight, chosen_value_weight, gate_weight, cosine, sine,
        chosen, code,
    )
    picked = pl.pallas_call(
        pick_kernel,
        name="pick",
        out_shape=shape_of((PEERS, CAP * BLK, 128), bf16),
        in_specs=[SMEM, VMEM, VMEM],
        out_specs=VMEM,
        scratch_shapes=[
            pltpu.VMEM((PEERS, 128), jnp.int32),
            pltpu.SMEM((PEERS, 128), jnp.int32),
            pltpu.SemaphoreType.DMA,
        ],
    )(rank, arrived, pairs)
    fetched = lax.all_to_all(picked, "kv", 0, 0, tiled=True)
    last_cos, last_sin = tables(jnp.arange(PEERS, dtype=jnp.int32) * TOK + (TOK + CMP_STRIDE - 1))
    mixed = pl.pallas_call(
        compressed_kernel,
        name="compressed",
        out_shape=shape_of((TOK, HEADS * HD), f32),
        in_specs=[SMEM] + [VMEM] * 7,
        out_specs=VMEM,
        scratch_shapes=[
            pltpu.VMEM((PEERS * NSUM, 128), bf16),
            pltpu.VMEM((PEERS * NSUM, 128), bf16),
        ],
        cost_estimate=pl.CostEstimate(flops=10**10, bytes_accessed=3 * 10**6, transcendentals=0),
    )(rank, arrived, queries, gates, squeeze_key_out, squeeze_value_out, last_cos, last_sin)
    blended = pl.pallas_call(
        selected_kernel,
        name="selected",
        out_shape=shape_of((TOK, HEADS * HD), bf16),
        in_specs=[SMEM, ANY, ANY] + [VMEM] * 4,
        out_specs=VMEM,
        scratch_shapes=[
            pltpu.VMEM((PEERS * CAP * BLK + TOK, 128), bf16),
            pltpu.VMEM((NSEL * BLK, 128), bf16),
            pltpu.SemaphoreType.DMA((2,)),
        ],
        cost_estimate=pl.CostEstimate(flops=10**9, bytes_accessed=3 * 10**6, transcendentals=0),
    )(place, fetched.reshape(PEERS * CAP * BLK, 128), pairs, queries, gates, mixed, bound)
    part = dot(blended, output_weight).astype(bf16)
    arrived_parts = lax.all_to_all(part.reshape(8, TOK // 8, -1), "tp", 0, 0, tiled=True)
    return arrived_parts.astype(f32).sum(axis=0).astype(bf16)


def solution(mesh):
    return jax.shard_map(
        on_device,
        mesh=mesh,
        in_specs=(
            P("kv", None),
            P(None, "tp"),
            P(None, "tp"),
            P(None, "tp"),
            P(None, "tp"),
            P(None, "tp"),
            P(),
            P(),
            P(),
            P(),
            P(None, None, "tp"),
            P("tp", None),
            P("tp", "kv", None),
        ),
        out_specs=P(("kv", "tp"), None),
        check_vma=False,
    )
```

```python
import jax
import jax.numpy as jnp
import numpy as np
from jax import lax
from jax.experimental import pallas as pl
from jax.experimental.pallas import tpu as pltpu
from jax.sharding import PartitionSpec as P


HD = 64
CMP_STRIDE = 16
BLK = 32
NSEL = 16
CAP = 4
ROTARY_BASE = 10000.0
NEG = -1e30
FLOOR = -1e29
TOK = 512
PEERS = 32
NSUM = 32
ROWS = 40
QB = TOK // BLK
HEADS = 4
NBLK = PEERS * QB
UNUSED = 99.0
AT_ONCE = 4
CHIPS = 4
PER_CHIP = QB // CHIPS
CHUNKS = 2
PICK = 8
PART = 128
OUT_ROWS = TOK // 8

INVERSE = (ROTARY_BASE ** (-np.arange(HD // 2, dtype=np.float64) / (HD // 2))).astype(np.float32)
INVERSE_ROW = np.tile(INVERSE, 4)[None, :]
SIGN_ROW = np.tile(np.repeat(np.array([-1.0, 1.0], np.float32), HD // 2), 2)[None, :]

bf16 = jnp.bfloat16
f32 = jnp.float32


def dot(a, b):
    return jnp.dot(a, b, preferred_element_type=f32)


def dot_t(a, b):
    return lax.dot_general(a, b, (((1,), (1,)), ((), ())), preferred_element_type=f32)


def lanes_of(shape):
    return lax.broadcasted_iota(jnp.int32, shape, len(shape) - 1)


def rows_of(shape):
    return lax.broadcasted_iota(jnp.int32, shape, len(shape) - 2)


def turned(x, cosine, sine):
    lane = lanes_of(x.shape)
    swapped = jnp.where(lane % HD < HD // 2, pltpu.roll(x, 128 - HD // 2, 1), pltpu.roll(x, HD // 2, 1))
    return x * cosine + swapped * sine


def gelu(x):
    return 0.5 * x * (1.0 + jnp.tanh(np.float32(np.sqrt(2.0 / np.pi)) * (x + 0.044715 * (x * x * x))))


def squeeze_out(pre_k, pre_v, out_k, out_v, cosine, sine):
    hidden = jnp.concatenate([gelu(pre_k).astype(bf16), gelu(pre_v).astype(bf16)], 1)
    zero = jnp.zeros(out_k.shape, bf16)
    weight = jnp.concatenate(
        [jnp.concatenate([out_k, zero], 1), jnp.concatenate([zero, out_v], 1)], 0
    )
    both = dot_t(hidden, weight)
    return jnp.where(lanes_of(both.shape) < HD, turned(both, cosine, sine), both)


def summary_kernel(
    rank_ref, tokens_hbm, wk_hbm, wv_hbm, ink_hbm, inv_hbm, outk_hbm, outv_hbm, turn_hbm, chosen_hbm,
    payload_ref, code_ref,
    tokens_ref, weight_ref, ink_ref, inv_ref, outk_ref, outv_ref, turn_ref, chosen_ref, raw_ref, sems,
):
    rank = rank_ref[0]
    part = TOK // CHUNKS
    copies = [
        (chosen_hbm, chosen_ref),
        (wk_hbm, weight_ref.at[:HD]),
        (wv_hbm, weight_ref.at[HD:]),
        *((tokens_hbm.at[pl.ds(c * part, part)], tokens_ref.at[pl.ds(c * part, part)]) for c in range(CHUNKS)),
        (ink_hbm, ink_ref),
        (inv_hbm, inv_ref),
        (outk_hbm, outk_ref),
        (outv_hbm, outv_ref),
        (turn_hbm, turn_ref),
    ]
    copies = [pltpu.make_async_copy(a, b, sems.at[n]) for n, (a, b) in enumerate(copies)]
    for copy in copies:
        copy.start()
    copies[0].wait()
    chosen = chosen_ref[...]
    query_block = rank * QB + rows_of(chosen.shape)
    wanted = jnp.where((chosen <= query_block) & (chosen // QB != rank), chosen, -1)
    every = lanes_of((QB, NBLK))
    hit = jnp.zeros((QB, NBLK), f32)
    for k in range(NSEL):
        hit = jnp.where(every == wanted[:, k : k + 1], 1.0, hit)
    present = jnp.broadcast_to(jnp.max(hit, 0, keepdims=True), (8, NBLK))
    lane = lanes_of((8, NBLK))
    running = present
    for step in (1, 2, 4, 8):
        running = running + jnp.where(lane % QB >= step, pltpu.roll(running, step, 1), 0.0)
    code = jnp.where(present > 0.0, running - present, UNUSED)
    code_ref[...] = code
    copies[1].wait()
    copies[2].wait()
    for c in range(CHUNKS):
        copies[3 + c].wait()
        rows = slice(c * part, c * part + part)
        raw_ref[rows] = dot_t(tokens_ref[rows], weight_ref[...]).astype(bf16).astype(f32)
    for copy in copies[3 + CHUNKS :]:
        copy.wait()
    ends = (rank * NSUM + rows_of((NSUM, 128))) * CMP_STRIDE + 2 * CMP_STRIDE - 1
    angles = ends.astype(f32) * turn_ref[:1]
    cosine = jnp.cos(angles)
    sine = jnp.sin(angles) * turn_ref[1:]
    zero = jnp.zeros((HD, 128), bf16)
    total = jnp.zeros((NSUM, 512), f32)
    for p in range(0, CMP_STRIDE, 2):
        left = []
        right = []
        for q in (p, p + 1):
            left.append(raw_ref[pl.ds(q, NSUM, stride=CMP_STRIDE), :].astype(bf16))
            low = pl.ds(q * HD, HD)
            high = pl.ds((q + CMP_STRIDE) * HD, HD)
            right.append(jnp.concatenate([ink_ref[low, :], ink_ref[high, :], zero, zero], 1))
            right.append(jnp.concatenate([zero, zero, inv_ref[low, :], inv_ref[high, :]], 1))
        total = total + dot(jnp.concatenate(left, 1), jnp.concatenate(right, 0))
    low_k, high_k = total[:, :128], total[:, 128:256]
    low_v, high_v = total[:, 256:384], total[:, 384:]
    pre_k = low_k + pltpu.roll(high_k, NSUM - 1, 0)
    pre_v = low_v + pltpu.roll(high_v, NSUM - 1, 0)
    summaries = squeeze_out(
        pre_k, pre_v, outk_ref[...], outv_ref[...], cosine, sine
    )
    payload = jnp.concatenate(
        [
            summaries,
            low_k[NSUM - 1 :], low_v[NSUM - 1 :], high_k[:1], high_v[:1],
            code[:1, :128], code[:1, 128:256], code[:1, 256:384], code[:1, 384:],
        ],
        0,
    ).astype(bf16)
    for peer in range(PEERS):
        payload_ref[peer] = payload


def project_kernel(
    rank_ref, tokens_ref, wq_ref, wk_ref, wv_ref, gate_ref, cos_ref, sin_ref, chosen_ref, code_ref,
    query_ref, pair_ref, gates_ref, place_ref, bound_ref,
    weight_ref,
):
    @pl.when(pl.program_id(0) == 0)
    def _():
        weight_ref[:HD] = wk_ref[...]
        weight_ref[HD : 2 * HD] = wv_ref[...]
        weight_ref[2 * HD :] = jnp.concatenate([gate_ref[0], gate_ref[1]], 0)
        rank = rank_ref[0]
        chosen = chosen_ref[...]
        query_block = rank * QB + rows_of(chosen.shape)
        code = code_ref[...]
        code = jnp.concatenate([code, code], 0)
        every = lanes_of((QB, NBLK))
        slot_lane = lanes_of((QB, NSEL))
        slot = jnp.zeros((QB, NSEL), f32)
        for k in range(NSEL):
            found = jnp.where(every == chosen[:, k : k + 1], code, 0.0)
            slot = jnp.where(slot_lane == k, jnp.sum(found, 1, keepdims=True), slot)
        holder = chosen // QB
        place = jnp.where(
            holder == rank, PEERS * CAP + chosen % QB, holder * CAP + slot.astype(jnp.int32)
        )
        place_ref[...] = jnp.where(chosen <= query_block, place, PEERS * CAP)
        order = jnp.where(chosen < query_block, -1.0, jnp.where(chosen > query_block, 1.0, 0.0))
        spread = (lanes_of((NSEL, NSEL * BLK)) // BLK == rows_of((NSEL, NSEL * BLK))).astype(bf16)
        inner = (lanes_of((QB, NSEL * BLK)) % BLK).astype(f32)
        bound_ref[...] = dot(order.astype(bf16), spread) * 64.0 + inner

    tokens = tokens_ref[...]
    cosine = cos_ref[...]
    sine = sin_ref[...]
    lane = lanes_of(cosine.shape)
    both = dot_t(tokens, weight_ref[...])
    pair = both[:, : 2 * HD]
    pair_ref[...] = jnp.where(lane < HD, turned(pair, cosine, sine), pair).astype(bf16)
    gates_ref[...] = jax.nn.sigmoid(both[:, 2 * HD :])
    queries = dot(tokens, wq_ref[...]) * np.float32(HD ** -0.5)
    for side in range(2):
        both = turned(queries[:, 128 * side : 128 * side + 128], cosine, sine)
        for half in range(2):
            head = 2 * side + half
            one = both if half == 0 else pltpu.roll(both, HD, 1)
            one = jnp.where(lane < HD, one, 0.0).astype(bf16)
            for b in range(PART // BLK):
                query_ref[b, head * BLK : (head + 1) * BLK, :] = one[b * BLK : (b + 1) * BLK]


def pick_kernel(rank_ref, arrived_ref, pair_hbm, picked_ref, pair_ref, ids_ref, ids_smem, sems):
    rank = rank_ref[0]
    step = pl.program_id(0)

    @pl.when(step == 0)
    def _():
        load = pltpu.make_async_copy(pair_hbm, pair_ref, sems.at[0])
        load.start()
        flat = arrived_ref[...].reshape(PEERS * ROWS, 128)
        shape = (PEERS, PEERS * ROWS)
        chosen_row = (lanes_of(shape) == rows_of(shape) * ROWS + NSUM + 4 + rank // 8).astype(bf16)
        codes = dot(chosen_row, flat)
        lane = lanes_of((PEERS, 128))
        mine = lane // QB == rank % 8
        inner = (lane % QB).astype(f32)
        ids = jnp.zeros((PEERS, 128), f32)
        for s in range(CAP):
            value = jnp.sum(jnp.where(mine & (codes == float(s)), inner, 0.0), 1, keepdims=True)
            ids = jnp.where(lane == s, value, ids)
        ids_ref[...] = ids.astype(jnp.int32)
        copy = pltpu.make_async_copy(ids_ref, ids_smem, sems.at[1])
        copy.start()
        load.wait()
        copy.wait()

    for peer in range(PICK):
        for s in range(CAP):
            start = pl.multiple_of(ids_smem[step * PICK + peer, s] * BLK, BLK)
            picked_ref[peer, s * BLK : (s + 1) * BLK, :] = pair_ref[pl.ds(start, BLK), :]


def mixed_heads(result, gates, first):
    lane = lanes_of((BLK, 128))
    halves = []
    for pair in range(2):
        gated = []
        for head in (2 * pair, 2 * pair + 1):
            gate = gates[:, first + head : first + head + 1]
            gated.append(result[head * BLK : (head + 1) * BLK] * gate)
        halves.append(jnp.where(lane < HD, pltpu.roll(gated[0], HD, 1), gated[1]))
    return halves


def compressed_kernel(
    rank_ref, arrived_ref, query_ref, gates_ref, outk_ref, outv_ref, cos_ref, sin_ref,
    mixed_ref, key_ref, value_ref,
):
    rank = rank_ref[0]
    flat = arrived_ref[...].reshape(PEERS * ROWS, 128)
    shape = (4 * PEERS, PEERS * ROWS)
    row = rows_of(shape)
    kind = row // PEERS
    source = row % PEERS + kind % 2
    target = source * ROWS + NSUM + jnp.where(kind == 0, 0, jnp.where(kind == 1, 2, jnp.where(kind == 2, 1, 3)))
    edges = dot(((lanes_of(shape) == target) & (source < PEERS)).astype(bf16), flat)
    pre_k = edges[:PEERS] + edges[PEERS : 2 * PEERS]
    pre_v = edges[2 * PEERS : 3 * PEERS] + edges[3 * PEERS :]
    last = squeeze_out(pre_k, pre_v, outk_ref[...], outv_ref[...], cos_ref[...], sin_ref[...])
    is_last = rows_of((NSUM, 128)) == NSUM - 1
    lane = lanes_of((NSUM, 128))
    for peer in range(PEERS):
        chunk = arrived_ref[peer, :NSUM, :].astype(f32)
        chunk = jnp.where(is_last, last[peer : peer + 1], chunk)
        value_ref[peer * NSUM : (peer + 1) * NSUM, :] = jnp.where(lane < HD, 1.0, chunk).astype(bf16)
        key_ref[peer * NSUM : (peer + 1) * NSUM, :] = chunk.astype(bf16)
    columns = lanes_of((HEADS * BLK, PEERS * NSUM))
    inside = lax.broadcasted_iota(jnp.int32, (HEADS * BLK, 1), 0) % BLK

    def some_blocks(step, carry):
        for j in range(AT_ONCE):
            b = step * AT_ONCE + j
            scores = dot_t(query_ref[b], key_ref[...])
            limit = (rank * TOK + b * BLK + inside - (2 * CMP_STRIDE - 1)) >> 4
            scores = jnp.where(columns <= limit, scores, NEG)
            largest = jnp.maximum(jnp.max(scores, 1, keepdims=True), FLOOR)
            weights = jnp.exp(scores - largest).astype(bf16)
            result = dot(weights, value_ref[...])
            result = result / jnp.maximum(pltpu.roll(result, HD, 1), 1.0)
            start = pl.multiple_of(b * BLK, BLK)
            halves = mixed_heads(result, gates_ref[pl.ds(start, BLK), :], 0)
            mixed_ref[pl.ds(start, BLK), :128] = halves[0].astype(bf16)
            mixed_ref[pl.ds(start, BLK), 128:] = halves[1].astype(bf16)
        return carry

    lax.fori_loop(0, QB // AT_ONCE, some_blocks, 0)


def selected_kernel(
    rank_ref, place_ref, fetched_hbm, pair_hbm, query_hbm, gates_hbm, mixed_hbm, bound_hbm,
    out0_ref, out1_ref, out2_ref, out3_ref,
    fetched_ref, pair_ref, query_ref, gates_ref, mixed_ref, bound_ref, key_ref, out_ref, sems,
):
    chip = rank_ref[1]
    copies = [
        (fetched_hbm, fetched_ref),
        (pair_hbm, pair_ref),
        (bound_hbm, bound_ref),
        (query_hbm, query_ref),
        (gates_hbm, gates_ref),
        (mixed_hbm, mixed_ref),
    ]
    copies = [pltpu.make_async_copy(a, b, sems.at[n]) for n, (a, b) in enumerate(copies)]
    for copy in copies:
        copy.start()
    inside = (lax.broadcasted_iota(jnp.int32, (HEADS * BLK, 1), 0) % BLK).astype(f32)
    lane = lanes_of((NSEL * BLK, 128))
    for copy in copies:
        copy.wait()

    def one_chip(d, carry):
        first = ((chip + d) % CHIPS) * PER_CHIP
        for j in range(PER_CHIP):
            b = first + j
            for k in range(NSEL):
                place = place_ref[b, k]
                far_row = pl.multiple_of(jnp.minimum(place, PEERS * CAP - 1) * BLK, BLK)
                near_row = pl.multiple_of(jnp.maximum(place - PEERS * CAP, 0) * BLK, BLK)
                is_near = jnp.full((BLK, 128), place, jnp.int32) >= PEERS * CAP
                key_ref[j, k * BLK : (k + 1) * BLK, :] = jnp.where(
                    is_near, pair_ref[pl.ds(near_row, BLK), :], fetched_ref[pl.ds(far_row, BLK), :]
                )
        for j in range(PER_CHIP):
            b = first + j
            keys = key_ref[j]
            scores = dot_t(query_ref[b], keys)
            scores = jnp.where(bound_ref[pl.ds(b, 1), :] <= inside, scores, NEG)
            largest = jnp.max(scores, 1, keepdims=True)
            weights = jnp.exp(scores - largest).astype(bf16)
            values = jnp.where(lane < HD, jnp.ones_like(keys), keys)
            result = dot(weights, values)
            result = result / pltpu.roll(result, HD, 1)
            start = pl.multiple_of(b * BLK, BLK)
            halves = mixed_heads(result, gates_ref[pl.ds(start, BLK), :], HEADS)
            for side in range(2):
                cols = slice(128 * side, 128 * side + 128)
                out_ref[d, j * BLK : (j + 1) * BLK, cols] = (
                    mixed_ref[pl.ds(start, BLK), cols] + halves[side]
                ).astype(bf16)
        return carry

    lax.fori_loop(0, CHIPS, one_chip, 0)
    for d, ref in enumerate((out0_ref, out1_ref, out2_ref, out3_ref)):
        ref[...] = out_ref[d]


def output_kernel(
    rank_ref, a0_ref, a1_ref, a2_ref, a3_ref, w0_ref, w1_ref, w2_ref, w3_ref,
    mine_ref, other_ref, sum_ref,
):
    core = rank_ref[2]
    total = dot(a0_ref[...], w0_ref[...])
    total = total + dot(a1_ref[...], w1_ref[...])
    total = total + dot(a3_ref[...], w3_ref[...])
    total = total + dot(a2_ref[...], w2_ref[...])
    sum_ref[...] = total
    mine_ref[...] = sum_ref[pl.ds(pl.multiple_of(core * OUT_ROWS, OUT_ROWS), OUT_ROWS), :]
    other = pl.multiple_of((1 - core) * OUT_ROWS, OUT_ROWS)
    other_ref[...] = sum_ref[pl.ds(other, OUT_ROWS), :].astype(bf16)


VMEM = pl.BlockSpec(memory_space=pltpu.VMEM)
SMEM = pl.BlockSpec(memory_space=pltpu.SMEM)
HBM = pl.BlockSpec(memory_space=pltpu.HBM)


def shape_of(shape, dtype):
    return jax.ShapeDtypeStruct(shape, dtype)


def stored(shape, dtype):
    return pltpu.HBM(shape, dtype)


def far(*values):
    return [pltpu.with_memory_space_constraint(value, pltpu.HBM) for value in values]


def limit(mib):
    return pltpu.CompilerParams(vmem_limit_bytes=mib * 1024 * 1024)


def around(value, distance):
    route = [(2 * y + c, 2 * ((y + distance) % CHIPS) + c) for y in range(CHIPS) for c in range(2)]
    return lax.ppermute(value, "tp", route)


def tables(positions):
    angles = positions.astype(f32)[:, None] * jnp.asarray(INVERSE_ROW)
    return jnp.cos(angles), jnp.sin(angles) * jnp.asarray(SIGN_ROW)


def on_device(
    tokens, query_weight, chosen_key_weight, chosen_value_weight, summary_key_weight,
    summary_value_weight, squeeze_key_in, squeeze_key_out, squeeze_value_in, squeeze_value_out,
    gate_weight, output_weight, chosen_blocks,
):
    kv_rank = lax.axis_index("kv")
    tp_rank = lax.axis_index("tp")
    rank = jnp.stack([kv_rank, tp_rank // 2, tp_rank % 2]).astype(jnp.int32)
    chosen = chosen_blocks[0]
    chosen_key_t = chosen_key_weight.T
    chosen_value_t = chosen_value_weight.T
    squeeze_key_t = squeeze_key_out.T
    squeeze_value_t = squeeze_value_out.T
    gate_t = gate_weight.transpose(0, 2, 1)
    turn = jnp.asarray(np.concatenate([INVERSE_ROW, SIGN_ROW], 0))
    payload, code = pl.pallas_call(
        summary_kernel,
        name="summaries",
        out_shape=(shape_of((PEERS, ROWS, 128), bf16), shape_of((8, NBLK), f32)),
        in_specs=[SMEM] + [HBM] * 9,
        out_specs=(VMEM, VMEM),
        scratch_shapes=[
            pltpu.VMEM((TOK, 2048), bf16),
            pltpu.VMEM((2 * HD, 2048), bf16),
            pltpu.VMEM((2048, 128), bf16),
            pltpu.VMEM((2048, 128), bf16),
            pltpu.VMEM((HD, 128), bf16),
            pltpu.VMEM((HD, 128), bf16),
            pltpu.VMEM((2, 128), f32),
            pltpu.VMEM((QB, NSEL), jnp.int32),
            pltpu.VMEM((TOK, 128), f32),
            pltpu.SemaphoreType.DMA((8 + CHUNKS,)),
        ],
        compiler_params=limit(16),
        cost_estimate=pl.CostEstimate(flops=10**9, bytes_accessed=5 * 10**6, transcendentals=0),
    )(
        rank,
        *far(
            tokens, summary_key_weight.T, summary_value_weight.T, squeeze_key_in, squeeze_value_in,
            squeeze_key_t, squeeze_value_t, turn, chosen,
        ),
    )
    weight_1 = around(output_weight, 1)
    weight_3 = around(output_weight, -1)
    arrived = lax.all_to_all(payload, "kv", 0, 0, tiled=True)
    cosine, sine = tables(kv_rank * TOK + jnp.arange(TOK, dtype=jnp.int32))
    queries, pairs, gates, place, bound = pl.pallas_call(
        project_kernel,
        name="projections",
        out_shape=(
            stored((QB, HEADS * BLK, 128), bf16),
            stored((TOK, 128), bf16),
            stored((TOK, 2 * HEADS), f32),
            stored((QB, NSEL), jnp.int32),
            stored((QB, NSEL * BLK), f32),
        ),
        grid=(TOK // PART,),
        in_specs=[
            SMEM,
            pl.BlockSpec((PART, 2048), lambda n: (n, 0)),
            VMEM, VMEM, VMEM, VMEM,
            pl.BlockSpec((PART, 128), lambda n: (n, 0)),
            pl.BlockSpec((PART, 128), lambda n: (n, 0)),
            VMEM, VMEM,
        ],
        out_specs=(
            pl.BlockSpec((PART // BLK, HEADS * BLK, 128), lambda n: (n, 0, 0)),
            pl.BlockSpec((PART, 128), lambda n: (n, 0)),
            pl.BlockSpec((PART, 2 * HEADS), lambda n: (n, 0)),
            VMEM, VMEM,
        ),
        scratch_shapes=[pltpu.VMEM((2 * HD + 2 * HEADS, 2048), bf16)],
        compiler_params=limit(20),
        cost_estimate=pl.CostEstimate(flops=10**10, bytes_accessed=5 * 10**6, transcendentals=0),
    )(
        rank,
        *far(tokens, query_weight, chosen_key_t, chosen_value_t),
        gate_t, cosine, sine, chosen, code,
    )
    picked = pl.pallas_call(
        pick_kernel,
        name="pick",
        out_shape=shape_of((PEERS, CAP * BLK, 128), bf16),
        grid=(PEERS // PICK,),
        in_specs=[SMEM, VMEM, HBM],
        out_specs=pl.BlockSpec((PICK, CAP * BLK, 128), lambda step: (step, 0, 0)),
        scratch_shapes=[
            pltpu.VMEM((TOK, 128), bf16),
            pltpu.VMEM((PEERS, 128), jnp.int32),
            pltpu.SMEM((PEERS, 128), jnp.int32),
            pltpu.SemaphoreType.DMA((2,)),
        ],
        compiler_params=limit(8),
    )(rank, arrived, *far(pairs))
    fetched = lax.all_to_all(picked, "kv", 0, 0, tiled=True)
    last_cos, last_sin = tables(jnp.arange(PEERS, dtype=jnp.int32) * TOK + (TOK + CMP_STRIDE - 1))
    mixed = pl.pallas_call(
        compressed_kernel,
        name="compressed",
        out_shape=stored((TOK, HEADS * HD), bf16),
        in_specs=[SMEM] + [VMEM] * 7,
        out_specs=VMEM,
        scratch_shapes=[
            pltpu.VMEM((PEERS * NSUM, 128), bf16),
            pltpu.VMEM((PEERS * NSUM, 128), bf16),
        ],
        compiler_params=limit(16),
        cost_estimate=pl.CostEstimate(flops=10**10, bytes_accessed=3 * 10**6, transcendentals=0),
    )(rank, arrived, *far(queries, gates), squeeze_key_t, squeeze_value_t, last_cos, last_sin)
    weight_1, mixed = lax.optimization_barrier((weight_1, mixed))
    weight_2 = around(weight_1, 1)

    pieces = pl.pallas_call(
        selected_kernel,
        name="selected",
        out_shape=(shape_of((PER_CHIP * BLK, HEADS * HD), bf16),) * CHIPS,
        in_specs=[SMEM, SMEM] + [HBM] * 6,
        out_specs=(VMEM,) * CHIPS,
        scratch_shapes=[
            pltpu.VMEM((PEERS * CAP * BLK, 128), bf16),
            pltpu.VMEM((TOK, 128), bf16),
            pltpu.VMEM((QB, HEADS * BLK, 128), bf16),
            pltpu.VMEM((TOK, 2 * HEADS), f32),
            pltpu.VMEM((TOK, HEADS * HD), bf16),
            pltpu.VMEM((QB, NSEL * BLK), f32),
            pltpu.VMEM((PER_CHIP, NSEL * BLK, 128), bf16),
            pltpu.VMEM((CHIPS, PER_CHIP * BLK, HEADS * HD), bf16),
            pltpu.SemaphoreType.DMA((6,)),
        ],
        compiler_params=limit(16),
        cost_estimate=pl.CostEstimate(flops=10**9, bytes_accessed=3 * 10**6, transcendentals=0),
    )(
        rank, place,
        *far(fetched.reshape(PEERS * CAP * BLK, 128), pairs, queries, gates, mixed, bound),
    )
    piece_2 = around(pieces[2], 2)
    piece_1 = around(pieces[1], 1)
    piece_3 = around(pieces[3], -1)
    mine, other = pl.pallas_call(
        output_kernel,
        name="output",
        out_shape=(shape_of((OUT_ROWS, 2048), f32), shape_of((OUT_ROWS, 2048), bf16)),
        in_specs=[SMEM] + [VMEM] * 8,
        out_specs=(VMEM, VMEM),
        scratch_shapes=[pltpu.VMEM((2 * OUT_ROWS, 2048), f32)],
        compiler_params=limit(16),
    )(
        rank, pieces[0], piece_1, piece_2, piece_3, output_weight, weight_1, weight_2, weight_3,
    )
    swapped = lax.ppermute(other, "tp", [(i, i ^ 1) for i in range(2 * CHIPS)])
    return (mine + swapped.astype(f32)).astype(bf16)


def solution(mesh):
    return jax.shard_map(
        on_device,
        mesh=mesh,
        in_specs=(
            P("kv", None),
            P(None, "tp"),
            P(None, "tp"),
            P(None, "tp"),
            P(None, "tp"),
            P(None, "tp"),
            P(),
            P(),
            P(),
            P(),
            P(None, None, "tp"),
            P("tp", None),
            P("tp", "kv", None),
        ),
        out_specs=P(("kv", "tp"), None),
        check_vma=False,
    )
```

```python
import jax
import jax.numpy as jnp
import numpy as np
from jax import lax
from jax.experimental import pallas as pl
from jax.experimental.pallas import tpu as pltpu
from jax.sharding import PartitionSpec as P


HD = 64
CMP_STRIDE = 16
BLK = 32
NSEL = 16
CAP = 4
ROTARY_BASE = 10000.0
NEG = -1e30
FLOOR = -1e29
TOK = 512
PEERS = 32
NSUM = 32
ROWS = 40
QB = TOK // BLK
HEADS = 4
NBLK = PEERS * QB
UNUSED = 99.0
COMPRESSED = 4
CHIPS = 4
PER_CHIP = QB // CHIPS
CHUNKS = 2
PICK = 16
PART = 256
GATHERED = 8
WEIGHED = 4
MIXED = 8
OUT_ROWS = TOK // 8

INVERSE = (ROTARY_BASE ** (-np.arange(HD // 2, dtype=np.float64) / (HD // 2))).astype(np.float32)
INVERSE_ROW = np.tile(INVERSE, 4)[None, :]
SIGN_ROW = np.tile(np.repeat(np.array([-1.0, 1.0], np.float32), HD // 2), 2)[None, :]

bf16 = jnp.bfloat16
f32 = jnp.float32


def dot(a, b):
    return jnp.dot(a, b, preferred_element_type=f32)


def dot_t(a, b):
    return lax.dot_general(a, b, (((1,), (1,)), ((), ())), preferred_element_type=f32)


def lanes_of(shape):
    return lax.broadcasted_iota(jnp.int32, shape, len(shape) - 1)


def rows_of(shape):
    return lax.broadcasted_iota(jnp.int32, shape, len(shape) - 2)


def turned(x, cosine, sine):
    lane = lanes_of(x.shape)
    swapped = jnp.where(lane % HD < HD // 2, pltpu.roll(x, 128 - HD // 2, 1), pltpu.roll(x, HD // 2, 1))
    return x * cosine + swapped * sine


def turns(positions, turn_ref):
    angles = positions.astype(f32) * turn_ref[:1]
    return jnp.cos(angles), jnp.sin(angles) * turn_ref[1:]


def gelu(x):
    return 0.5 * x * (1.0 + jnp.tanh(np.float32(np.sqrt(2.0 / np.pi)) * (x + 0.044715 * (x * x * x))))


def squeeze_out(pre_k, pre_v, out_k, out_v, cosine, sine):
    hidden = jnp.concatenate([gelu(pre_k).astype(bf16), gelu(pre_v).astype(bf16)], 1)
    zero = jnp.zeros(out_k.shape, bf16)
    weight = jnp.concatenate(
        [jnp.concatenate([out_k, zero], 1), jnp.concatenate([zero, out_v], 1)], 0
    )
    both = dot_t(hidden, weight)
    return jnp.where(lanes_of(both.shape) < HD, turned(both, cosine, sine), both)


def summary_kernel(
    tokens_hbm, wk_hbm, wv_hbm, ink_hbm, inv_hbm, outk_hbm, outv_hbm, turn_hbm, chosen_hbm,
    payload_ref, code_ref,
    tokens_ref, weight_ref, ink_ref, inv_ref, outk_ref, outv_ref, turn_ref, chosen_ref, raw_ref, sems,
):
    rank = lax.axis_index("kv")
    part = TOK // CHUNKS
    copies = [
        (chosen_hbm, chosen_ref),
        (wk_hbm, weight_ref.at[:HD]),
        (wv_hbm, weight_ref.at[HD:]),
        *((tokens_hbm.at[pl.ds(c * part, part)], tokens_ref.at[pl.ds(c * part, part)]) for c in range(CHUNKS)),
        (ink_hbm, ink_ref),
        (inv_hbm, inv_ref),
        (outk_hbm, outk_ref),
        (outv_hbm, outv_ref),
        (turn_hbm, turn_ref),
    ]
    copies = [pltpu.make_async_copy(a, b, sems.at[n]) for n, (a, b) in enumerate(copies)]
    for copy in copies:
        copy.start()
    copies[0].wait()
    chosen = chosen_ref[...]
    query_block = rank * QB + rows_of(chosen.shape)
    wanted = jnp.where((chosen <= query_block) & (chosen // QB != rank), chosen, -1)
    every = lanes_of((QB, NBLK))
    hit = jnp.zeros((QB, NBLK), f32)
    for k in range(NSEL):
        hit = jnp.where(every == wanted[:, k : k + 1], 1.0, hit)
    present = jnp.broadcast_to(jnp.max(hit, 0, keepdims=True), (8, NBLK))
    lane = lanes_of((8, NBLK))
    running = present
    for step in (1, 2, 4, 8):
        running = running + jnp.where(lane % QB >= step, pltpu.roll(running, step, 1), 0.0)
    code = jnp.where(present > 0.0, running - present, UNUSED)
    code_ref[...] = code
    copies[1].wait()
    copies[2].wait()
    for c in range(CHUNKS):
        copies[3 + c].wait()
        rows = slice(c * part, c * part + part)
        raw_ref[rows] = dot_t(tokens_ref[rows], weight_ref[...]).astype(bf16).astype(f32)
    for copy in copies[3 + CHUNKS :]:
        copy.wait()
    ends = (rank * NSUM + rows_of((NSUM, 128))) * CMP_STRIDE + 2 * CMP_STRIDE - 1
    cosine, sine = turns(ends, turn_ref)
    zero = jnp.zeros((HD, 128), bf16)
    total = jnp.zeros((NSUM, 512), f32)
    for p in range(0, CMP_STRIDE, 2):
        left = []
        right = []
        for q in (p, p + 1):
            left.append(raw_ref[pl.ds(q, NSUM, stride=CMP_STRIDE), :].astype(bf16))
            low = pl.ds(q * HD, HD)
            high = pl.ds((q + CMP_STRIDE) * HD, HD)
            right.append(jnp.concatenate([ink_ref[low, :], ink_ref[high, :], zero, zero], 1))
            right.append(jnp.concatenate([zero, zero, inv_ref[low, :], inv_ref[high, :]], 1))
        total = total + dot(jnp.concatenate(left, 1), jnp.concatenate(right, 0))
    low_k, high_k = total[:, :128], total[:, 128:256]
    low_v, high_v = total[:, 256:384], total[:, 384:]
    pre_k = low_k + pltpu.roll(high_k, NSUM - 1, 0)
    pre_v = low_v + pltpu.roll(high_v, NSUM - 1, 0)
    summaries = squeeze_out(
        pre_k, pre_v, outk_ref[...], outv_ref[...], cosine, sine
    )
    payload = jnp.concatenate(
        [
            summaries,
            low_k[NSUM - 1 :], low_v[NSUM - 1 :], high_k[:1], high_v[:1],
            code[:1, :128], code[:1, 128:256], code[:1, 256:384], code[:1, 384:],
        ],
        0,
    ).astype(bf16)
    for peer in range(PEERS):
        payload_ref[peer] = payload


def pair_kernel(
    tokens_ref, wk_ref, wv_ref, gate_ref, cos_ref, sin_ref, pair_ref, gates_ref, weight_ref
):
    @pl.when(pl.program_id(0) == 0)
    def _():
        weight_ref[:HD] = wk_ref[...]
        weight_ref[HD : 2 * HD] = wv_ref[...]
        weight_ref[2 * HD :] = jnp.concatenate([gate_ref[0], gate_ref[1]], 0)

    both = dot_t(tokens_ref[...], weight_ref[...])
    pair = both[:, : 2 * HD]
    lane = lanes_of(pair.shape)
    pair_ref[...] = jnp.where(
        lane < HD, turned(pair, cos_ref[...], sin_ref[...]), pair
    ).astype(bf16)
    gates_ref[...] = jax.nn.sigmoid(both[:, 2 * HD :])


def query_kernel(
    tokens_ref, wq_ref, cos_ref, sin_ref, chosen_ref, code_ref,
    query_ref, place_ref, bound_ref,
):
    @pl.when(pl.program_id(0) == 0)
    def _():
        rank = lax.axis_index("kv")
        chosen = chosen_ref[...]
        query_block = rank * QB + rows_of(chosen.shape)
        code = code_ref[...]
        code = jnp.concatenate([code, code], 0)
        every = lanes_of((QB, NBLK))
        slot_lane = lanes_of((QB, NSEL))
        slot = jnp.zeros((QB, NSEL), f32)
        for k in range(NSEL):
            found = jnp.where(every == chosen[:, k : k + 1], code, 0.0)
            slot = jnp.where(slot_lane == k, jnp.sum(found, 1, keepdims=True), slot)
        holder = chosen // QB
        place = jnp.where(
            holder == rank, PEERS * CAP + chosen % QB, holder * CAP + slot.astype(jnp.int32)
        )
        place_ref[...] = jnp.where(chosen <= query_block, place, PEERS * CAP)
        order = jnp.where(chosen < query_block, -1.0, jnp.where(chosen > query_block, 1.0, 0.0))
        spread = (lanes_of((NSEL, NSEL * BLK)) // BLK == rows_of((NSEL, NSEL * BLK))).astype(bf16)
        inner = (lanes_of((QB, NSEL * BLK)) % BLK).astype(f32)
        bound_ref[...] = dot(order.astype(bf16), spread) * 64.0 + inner

    cosine = cos_ref[...]
    sine = sin_ref[...]
    lane = lanes_of(cosine.shape)
    queries = dot(tokens_ref[...], wq_ref[...]) * np.float32(HD ** -0.5)
    for side in range(2):
        both = turned(queries[:, 128 * side : 128 * side + 128], cosine, sine)
        for half in range(2):
            head = 2 * side + half
            one = both if half == 0 else pltpu.roll(both, HD, 1)
            one = jnp.where(lane < HD, one, 0.0).astype(bf16)
            for b in range(PART // BLK):
                query_ref[b, head * BLK : (head + 1) * BLK, :] = one[b * BLK : (b + 1) * BLK]


def pick_kernel(arrived_ref, pair_hbm, picked_ref, pair_ref, ids_ref, ids_smem, sems):
    rank = lax.axis_index("kv")
    step = pl.program_id(0)

    @pl.when(step == 0)
    def _():
        load = pltpu.make_async_copy(pair_hbm, pair_ref, sems.at[0])
        load.start()
        flat = arrived_ref[...].reshape(PEERS * ROWS, 128)
        shape = (PEERS, PEERS * ROWS)
        chosen_row = (lanes_of(shape) == rows_of(shape) * ROWS + NSUM + 4 + rank // 8).astype(bf16)
        codes = dot(chosen_row, flat)
        lane = lanes_of((PEERS, 128))
        mine = lane // QB == rank % 8
        inner = (lane % QB).astype(f32)
        ids = jnp.zeros((PEERS, 128), f32)
        for s in range(CAP):
            value = jnp.sum(jnp.where(mine & (codes == float(s)), inner, 0.0), 1, keepdims=True)
            ids = jnp.where(lane == s, value, ids)
        ids_ref[...] = ids.astype(jnp.int32)
        copy = pltpu.make_async_copy(ids_ref, ids_smem, sems.at[1])
        copy.start()
        load.wait()
        copy.wait()

    for peer in range(PICK):
        for s in range(CAP):
            start = pl.multiple_of(ids_smem[step * PICK + peer, s] * BLK, BLK)
            picked_ref[peer, s * BLK : (s + 1) * BLK, :] = pair_ref[pl.ds(start, BLK), :]


def mixed_heads(result, gates, first):
    lane = lanes_of((BLK, 128))
    halves = []
    for pair in range(2):
        gated = []
        for head in (2 * pair, 2 * pair + 1):
            gate = gates[:, first + head : first + head + 1]
            gated.append(result[head * BLK : (head + 1) * BLK] * gate)
        halves.append(jnp.where(lane < HD, pltpu.roll(gated[0], HD, 1), gated[1]))
    return halves


def compressed_kernel(
    arrived_ref, query_ref, gates_ref, outk_ref, outv_ref, turn_ref, mixed_ref,
    key_ref, value_ref, score_ref, weight_ref,
):
    rank = lax.axis_index("kv")
    flat = arrived_ref[...].reshape(PEERS * ROWS, 128)
    shape = (4 * PEERS, PEERS * ROWS)
    row = rows_of(shape)
    kind = row // PEERS
    source = row % PEERS + kind % 2
    target = source * ROWS + NSUM + jnp.where(kind == 0, 0, jnp.where(kind == 1, 2, jnp.where(kind == 2, 1, 3)))
    edges = dot(((lanes_of(shape) == target) & (source < PEERS)).astype(bf16), flat)
    pre_k = edges[:PEERS] + edges[PEERS : 2 * PEERS]
    pre_v = edges[2 * PEERS : 3 * PEERS] + edges[3 * PEERS :]
    ends = rows_of((PEERS, 128)) * TOK + TOK + CMP_STRIDE - 1
    last = squeeze_out(pre_k, pre_v, outk_ref[...], outv_ref[...], *turns(ends, turn_ref))
    is_last = rows_of((NSUM, 128)) == NSUM - 1
    lane = lanes_of((NSUM, 128))
    for peer in range(PEERS):
        chunk = arrived_ref[peer, :NSUM, :].astype(f32)
        chunk = jnp.where(is_last, last[peer : peer + 1], chunk)
        value_ref[peer * NSUM : (peer + 1) * NSUM, :] = jnp.where(lane < HD, 1.0, chunk).astype(bf16)
        key_ref[peer * NSUM : (peer + 1) * NSUM, :] = chunk.astype(bf16)
    group = COMPRESSED * HEADS * BLK
    columns = lanes_of((HEADS * BLK, PEERS * NSUM))
    inside = lax.broadcasted_iota(jnp.int32, (HEADS * BLK, 1), 0) % BLK

    def score(step, carry):
        rows = query_ref[pl.ds(step * COMPRESSED, COMPRESSED)].reshape(group, 128)
        score_ref[pl.ds(pl.multiple_of(step * group, group), group), :] = dot_t(rows, key_ref[...])
        return carry

    def weigh(step, carry):
        for j in range(COMPRESSED):
            b = step * COMPRESSED + j
            rows = pl.ds(pl.multiple_of(b * HEADS * BLK, HEADS * BLK), HEADS * BLK)
            limit = (rank * TOK + b * BLK + inside - (2 * CMP_STRIDE - 1)) >> 4
            scores = jnp.where(columns <= limit, score_ref[rows, :], NEG)
            largest = jnp.maximum(jnp.max(scores, 1, keepdims=True), FLOOR)
            weight_ref[rows, :] = jnp.exp(scores - largest).astype(bf16)
        return carry

    def mix(step, carry):
        rows = pl.ds(pl.multiple_of(step * group, group), group)
        result = dot(weight_ref[rows, :], value_ref[...])
        result = result / jnp.maximum(pltpu.roll(result, HD, 1), 1.0)
        for j in range(COMPRESSED):
            start = pl.multiple_of((step * COMPRESSED + j) * BLK, BLK)
            one = result[j * HEADS * BLK : (j + 1) * HEADS * BLK]
            halves = mixed_heads(one, gates_ref[pl.ds(start, BLK), :], 0)
            mixed_ref[pl.ds(start, BLK), :128] = halves[0].astype(bf16)
            mixed_ref[pl.ds(start, BLK), 128:] = halves[1].astype(bf16)
        return carry

    lax.fori_loop(0, QB // COMPRESSED, score, 0)
    lax.fori_loop(0, QB // COMPRESSED, weigh, 0)
    lax.fori_loop(0, QB // COMPRESSED, mix, 0)


def selected_kernel(
    place_hbm, fetched_hbm, pair_hbm, query_hbm, bound_hbm, gates_hbm, mixed_hbm,
    out0_ref, out1_ref, out2_ref, out3_ref,
    place_ref, fetched_ref, pair_ref, query_ref, bound_ref, gates_ref, mixed_ref,
    key_ref, score_ref, weight_ref, out_ref, sems,
):
    chip = lax.axis_index("tp") // 2
    copies = [
        (place_hbm, place_ref),
        (fetched_hbm, fetched_ref),
        (pair_hbm, pair_ref),
        (query_hbm, query_ref),
        (bound_hbm, bound_ref),
        (gates_hbm, gates_ref),
        (mixed_hbm, mixed_ref),
    ]
    copies = [pltpu.make_async_copy(a, b, sems.at[n]) for n, (a, b) in enumerate(copies)]
    for copy in copies:
        copy.start()
    inside = (lax.broadcasted_iota(jnp.int32, (HEADS * BLK, 1), 0) % BLK).astype(f32)
    lane = lanes_of((NSEL * BLK, 128))

    def score(step, carry):
        for j in range(GATHERED):
            b = step * GATHERED + j
            for k in range(NSEL):
                place = place_ref[b, k]
                far_row = pl.multiple_of(jnp.minimum(place, PEERS * CAP - 1) * BLK, BLK)
                near_row = pl.multiple_of(jnp.maximum(place - PEERS * CAP, 0) * BLK, BLK)
                is_near = jnp.full((BLK, 128), place, jnp.int32) >= PEERS * CAP
                key_ref[b, k * BLK : (k + 1) * BLK, :] = jnp.where(
                    is_near, pair_ref[pl.ds(near_row, BLK), :], fetched_ref[pl.ds(far_row, BLK), :]
                )
            score_ref[b] = dot_t(query_ref[b], key_ref[b])
        return carry

    def weigh(step, carry):
        for j in range(WEIGHED):
            b = step * WEIGHED + j
            scores = jnp.where(bound_ref[pl.ds(b, 1), :] <= inside, score_ref[b], NEG)
            largest = jnp.max(scores, 1, keepdims=True)
            weight_ref[b] = jnp.exp(scores - largest).astype(bf16)
        return carry

    def mix(step, carry):
        for j in range(MIXED):
            b = step * MIXED + j
            keys = key_ref[b]
            values = jnp.where(lane < HD, jnp.ones_like(keys), keys)
            result = dot(weight_ref[b], values)
            result = result / pltpu.roll(result, HD, 1)
            start = pl.multiple_of(b * BLK, BLK)
            halves = mixed_heads(result, gates_ref[pl.ds(start, BLK), :], HEADS)
            row = pl.multiple_of((b % PER_CHIP) * BLK, BLK)
            for side in range(2):
                cols = slice(128 * side, 128 * side + 128)
                out_ref[(b // PER_CHIP - chip + CHIPS) % CHIPS, pl.ds(row, BLK), cols] = (
                    mixed_ref[pl.ds(start, BLK), cols] + halves[side]
                ).astype(bf16)
        return carry

    for copy in copies[:4]:
        copy.wait()
    lax.fori_loop(0, QB // GATHERED, score, 0)
    copies[4].wait()
    lax.fori_loop(0, QB // WEIGHED, weigh, 0)
    copies[5].wait()
    copies[6].wait()
    lax.fori_loop(0, QB // MIXED, mix, 0)
    for d, ref in enumerate((out0_ref, out1_ref, out2_ref, out3_ref)):
        ref[...] = out_ref[d]


def output_kernel(
    a0_ref, a1_ref, a2_ref, a3_ref, w0_ref, w1_ref, w2a_ref, w2b_ref, w3_ref,
    mine_ref, other_ref, sum_ref,
):
    core = lax.axis_index("tp") % 2
    total = dot(a0_ref[...], w0_ref[...])
    total = total + dot(a1_ref[...], w1_ref[...])
    total = total + dot(a3_ref[...], w3_ref[...])
    half = HEADS * HD // 2
    total = total + dot(a2_ref[:, :half], w2a_ref[...])
    total = total + dot(a2_ref[:, half:], w2b_ref[...])
    sum_ref[...] = total
    mine_ref[...] = sum_ref[pl.ds(pl.multiple_of(core * OUT_ROWS, OUT_ROWS), OUT_ROWS), :]
    other = pl.multiple_of((1 - core) * OUT_ROWS, OUT_ROWS)
    other_ref[...] = sum_ref[pl.ds(other, OUT_ROWS), :].astype(bf16)


VMEM = pl.BlockSpec(memory_space=pltpu.VMEM)
SMEM = pl.BlockSpec(memory_space=pltpu.SMEM)
HBM = pl.BlockSpec(memory_space=pltpu.HBM)


def shape_of(shape, dtype):
    return jax.ShapeDtypeStruct(shape, dtype)


def stored(shape, dtype):
    return pltpu.HBM(shape, dtype)


def far(*values):
    return [pltpu.with_memory_space_constraint(value, pltpu.HBM) for value in values]


def limit(mib):
    return pltpu.CompilerParams(vmem_limit_bytes=mib * 1024 * 1024)


def around(value, distance):
    route = [(2 * y + c, 2 * ((y + distance) % CHIPS) + c) for y in range(CHIPS) for c in range(2)]
    return lax.ppermute(value, "tp", route)


def tables(positions):
    angles = positions.astype(f32)[:, None] * jnp.asarray(INVERSE_ROW)
    return jnp.cos(angles), jnp.sin(angles) * jnp.asarray(SIGN_ROW)


def on_device(
    tokens, query_weight, chosen_key_weight, chosen_value_weight, summary_key_weight,
    summary_value_weight, squeeze_key_in, squeeze_key_out, squeeze_value_in, squeeze_value_out,
    gate_weight, output_weight, chosen_blocks,
):
    kv_rank = lax.axis_index("kv")
    chosen = chosen_blocks[0]
    chosen_key_t = chosen_key_weight.T
    chosen_value_t = chosen_value_weight.T
    squeeze_key_t = squeeze_key_out.T
    squeeze_value_t = squeeze_value_out.T
    gate_t = gate_weight.transpose(0, 2, 1)
    turn = jnp.asarray(np.concatenate([INVERSE_ROW, SIGN_ROW], 0))
    payload, code = pl.pallas_call(
        summary_kernel,
        name="summaries",
        out_shape=(shape_of((PEERS, ROWS, 128), bf16), stored((8, NBLK), f32)),
        in_specs=[HBM] * 9,
        out_specs=(VMEM, VMEM),
        scratch_shapes=[
            pltpu.VMEM((TOK, 2048), bf16),
            pltpu.VMEM((2 * HD, 2048), bf16),
            pltpu.VMEM((2048, 128), bf16),
            pltpu.VMEM((2048, 128), bf16),
            pltpu.VMEM((HD, 128), bf16),
            pltpu.VMEM((HD, 128), bf16),
            pltpu.VMEM((2, 128), f32),
            pltpu.VMEM((QB, NSEL), jnp.int32),
            pltpu.VMEM((TOK, 128), f32),
            pltpu.SemaphoreType.DMA((8 + CHUNKS,)),
        ],
        compiler_params=limit(16),
        cost_estimate=pl.CostEstimate(flops=10**9, bytes_accessed=5 * 10**6, transcendentals=0),
    )(
        *far(
            tokens, summary_key_weight.T, summary_value_weight.T, squeeze_key_in, squeeze_value_in,
            squeeze_key_t, squeeze_value_t, turn, chosen,
        ),
    )
    weight_1 = around(output_weight, 1)
    weight_3 = around(output_weight, -1)
    arrived = lax.all_to_all(payload, "kv", 0, 0, tiled=True)
    cosine, sine = tables(kv_rank * TOK + jnp.arange(TOK, dtype=jnp.int32))
    row_block = pl.BlockSpec((PART, 128), lambda n: (n, 0))
    token_block = pl.BlockSpec((PART, 2048), lambda n: (n, 0))
    pairs, gates = pl.pallas_call(
        pair_kernel,
        name="pairs",
        out_shape=(stored((TOK, 128), bf16), stored((TOK, 2 * HEADS), f32)),
        grid=(TOK // PART,),
        in_specs=[token_block, VMEM, VMEM, VMEM, row_block, row_block],
        out_specs=(row_block, pl.BlockSpec((PART, 2 * HEADS), lambda n: (n, 0))),
        scratch_shapes=[pltpu.VMEM((2 * HD + 2 * HEADS, 2048), bf16)],
        compiler_params=limit(16),
        cost_estimate=pl.CostEstimate(flops=10**10, bytes_accessed=3 * 10**6, transcendentals=0),
    )(*far(tokens, chosen_key_t, chosen_value_t), gate_t, *far(cosine, sine))
    picked = pl.pallas_call(
        pick_kernel,
        name="pick",
        out_shape=shape_of((PEERS, CAP * BLK, 128), bf16),
        grid=(PEERS // PICK,),
        in_specs=[VMEM, HBM],
        out_specs=pl.BlockSpec((PICK, CAP * BLK, 128), lambda step: (step, 0, 0)),
        scratch_shapes=[
            pltpu.VMEM((TOK, 128), bf16),
            pltpu.VMEM((PEERS, 128), jnp.int32),
            pltpu.SMEM((PEERS, 128), jnp.int32),
            pltpu.SemaphoreType.DMA((2,)),
        ],
        compiler_params=limit(8),
    )(arrived, *far(pairs))
    fetched = lax.all_to_all(picked, "kv", 0, 0, tiled=True)
    queries, place, bound = pl.pallas_call(
        query_kernel,
        name="queries",
        out_shape=(
            stored((QB, HEADS * BLK, 128), bf16),
            stored((QB, NSEL), jnp.int32),
            stored((QB, NSEL * BLK), f32),
        ),
        grid=(TOK // PART,),
        in_specs=[
            token_block, VMEM, row_block, row_block, VMEM, VMEM,
        ],
        out_specs=(
            pl.BlockSpec((PART // BLK, HEADS * BLK, 128), lambda n: (n, 0, 0)),
            VMEM,
            VMEM,
        ),
        compiler_params=limit(16),
        cost_estimate=pl.CostEstimate(flops=10**10, bytes_accessed=3 * 10**6, transcendentals=0),
    )(*far(tokens, query_weight, cosine, sine, chosen, code))
    mixed = pl.pallas_call(
        compressed_kernel,
        name="compressed",
        out_shape=stored((TOK, HEADS * HD), bf16),
        in_specs=[VMEM] * 6,
        out_specs=VMEM,
        scratch_shapes=[
            pltpu.VMEM((PEERS * NSUM, 128), bf16),
            pltpu.VMEM((PEERS * NSUM, 128), bf16),
            pltpu.VMEM((QB * HEADS * BLK, PEERS * NSUM), f32),
            pltpu.VMEM((QB * HEADS * BLK, PEERS * NSUM), bf16),
        ],
        compiler_params=limit(24),
        cost_estimate=pl.CostEstimate(flops=10**10, bytes_accessed=3 * 10**6, transcendentals=0),
    )(arrived, *far(queries, gates, squeeze_key_t, squeeze_value_t, turn))
    weight_1, weight_3, mixed = lax.optimization_barrier((weight_1, weight_3, mixed))
    half = weight_1.shape[0] // 2
    weight_2a = around(weight_1[:half], 1)
    weight_2b = around(weight_3[half:], -1)
    pieces = pl.pallas_call(
        selected_kernel,
        name="selected",
        out_shape=(shape_of((PER_CHIP * BLK, HEADS * HD), bf16),) * CHIPS,
        in_specs=[HBM] * 7,
        out_specs=(VMEM,) * CHIPS,
        scratch_shapes=[
            pltpu.SMEM((QB, NSEL), jnp.int32),
            pltpu.VMEM((PEERS * CAP * BLK, 128), bf16),
            pltpu.VMEM((TOK, 128), bf16),
            pltpu.VMEM((QB, HEADS * BLK, 128), bf16),
            pltpu.VMEM((QB, NSEL * BLK), f32),
            pltpu.VMEM((TOK, 2 * HEADS), f32),
            pltpu.VMEM((TOK, HEADS * HD), bf16),
            pltpu.VMEM((QB, NSEL * BLK, 128), bf16),
            pltpu.VMEM((QB, HEADS * BLK, NSEL * BLK), f32),
            pltpu.VMEM((QB, HEADS * BLK, NSEL * BLK), bf16),
            pltpu.VMEM((CHIPS, PER_CHIP * BLK, HEADS * HD), bf16),
            pltpu.SemaphoreType.DMA((7,)),
        ],
        compiler_params=limit(24),
        cost_estimate=pl.CostEstimate(flops=10**9, bytes_accessed=3 * 10**6, transcendentals=0),
    )(
        *far(place, fetched.reshape(PEERS * CAP * BLK, 128), pairs, queries, bound, gates, mixed),
    )
    piece_2 = around(pieces[2], 2)
    piece_1 = around(pieces[1], 1)
    piece_3 = around(pieces[3], -1)
    mine, other = pl.pallas_call(
        output_kernel,
        name="output",
        out_shape=(shape_of((OUT_ROWS, 2048), f32), shape_of((OUT_ROWS, 2048), bf16)),
        in_specs=[VMEM] * 9,
        out_specs=(VMEM, VMEM),
        scratch_shapes=[pltpu.VMEM((2 * OUT_ROWS, 2048), f32)],
        compiler_params=limit(16),
    )(
        pieces[0], piece_1, piece_2, piece_3, output_weight, weight_1, weight_2a, weight_2b,
        weight_3,
    )
    swapped = lax.ppermute(other, "tp", [(i, i ^ 1) for i in range(2 * CHIPS)])
    return (mine + swapped.astype(f32)).astype(bf16)


def solution(mesh):
    return jax.shard_map(
        on_device,
        mesh=mesh,
        in_specs=(
            P("kv", None),
            P(None, "tp"),
            P(None, "tp"),
            P(None, "tp"),
            P(None, "tp"),
            P(None, "tp"),
            P(),
            P(),
            P(),
            P(),
            P(None, None, "tp"),
            P("tp", None),
            P("tp", "kv", None),
        ),
        out_specs=P(("kv", "tp"), None),
        check_vma=False,
    )
```

```python
import jax
import jax.numpy as jnp
import numpy as np
from jax import lax
from jax.experimental import pallas as pl
from jax.experimental.pallas import tpu as pltpu
from jax.sharding import Mesh
from jax.sharding import PartitionSpec as P


HD = 64
CMP_STRIDE = 16
BLK = 32
NSEL = 16
CAP = 4
ROTARY_BASE = 10000.0
NEG = -1e30
FLOOR = -1e29
TOK = 512
PEERS = 32
LAYERS = 8
COLUMNS = 4
NSUM = 32
ROWS = 40
QB = TOK // BLK
HEADS = 4
NBLK = PEERS * QB
UNUSED = 99.0
COMPRESSED = 4
CHIPS = 4
PER_CHIP = QB // CHIPS
CHUNKS = 2
PART = 256
SPLIT = 288
GATHERED = 8
WEIGHED = 4
MIXED = 8
OUT_ROWS = TOK // 8

INVERSE = (ROTARY_BASE ** (-np.arange(HD // 2, dtype=np.float64) / (HD // 2))).astype(np.float32)
INVERSE_ROW = np.tile(INVERSE, 4)[None, :]
SIGN_ROW = np.tile(np.repeat(np.array([-1.0, 1.0], np.float32), HD // 2), 2)[None, :]

bf16 = jnp.bfloat16
f32 = jnp.float32


def kv_index():
    return lax.axis_index("z") * COLUMNS + lax.axis_index("x")


def dot(a, b):
    return jnp.dot(a, b, preferred_element_type=f32)


def dot_t(a, b):
    return lax.dot_general(a, b, (((1,), (1,)), ((), ())), preferred_element_type=f32)


def lanes_of(shape):
    return lax.broadcasted_iota(jnp.int32, shape, len(shape) - 1)


def rows_of(shape):
    return lax.broadcasted_iota(jnp.int32, shape, len(shape) - 2)


def turned(x, cosine, sine):
    lane = lanes_of(x.shape)
    swapped = jnp.where(lane % HD < HD // 2, pltpu.roll(x, 128 - HD // 2, 1), pltpu.roll(x, HD // 2, 1))
    return x * cosine + swapped * sine


def turns(positions, turn_ref):
    angles = positions.astype(f32) * turn_ref[:1]
    return jnp.cos(angles), jnp.sin(angles) * turn_ref[1:]


def gelu(x):
    return 0.5 * x * (1.0 + jnp.tanh(np.float32(np.sqrt(2.0 / np.pi)) * (x + 0.044715 * (x * x * x))))


def squeeze_out(pre_k, pre_v, out_k, out_v, cosine, sine):
    hidden = jnp.concatenate([gelu(pre_k).astype(bf16), gelu(pre_v).astype(bf16)], 1)
    zero = jnp.zeros(out_k.shape, bf16)
    weight = jnp.concatenate(
        [jnp.concatenate([out_k, zero], 1), jnp.concatenate([zero, out_v], 1)], 0
    )
    both = dot_t(hidden, weight)
    return jnp.where(lanes_of(both.shape) < HD, turned(both, cosine, sine), both)


def token_kernel(
    tokens_hbm, wk_hbm, wv_hbm, ck_hbm, cv_hbm, ink_hbm, inv_hbm, outk_hbm, outv_hbm, turn_hbm,
    chosen_hbm, payload_ref, code_ref, cos_ref, sin_ref,
    tokens_ref, weight_ref, ink_ref, inv_ref, outk_ref, outv_ref, turn_ref, chosen_ref, raw_ref,
    coarse_ref, sems,
):
    rank = kv_index()
    part = TOK // CHUNKS
    copies = [
        (chosen_hbm, chosen_ref),
        (turn_hbm, turn_ref),
        (wk_hbm, weight_ref.at[:HD]),
        (wv_hbm, weight_ref.at[HD : 2 * HD]),
        (ck_hbm, weight_ref.at[2 * HD : 3 * HD]),
        (cv_hbm, weight_ref.at[3 * HD :]),
        *((tokens_hbm.at[pl.ds(c * part, part)], tokens_ref.at[pl.ds(c * part, part)]) for c in range(CHUNKS)),
        (ink_hbm, ink_ref),
        (inv_hbm, inv_ref),
        (outk_hbm, outk_ref),
        (outv_hbm, outv_ref),
    ]
    copies = [pltpu.make_async_copy(a, b, sems.at[n]) for n, (a, b) in enumerate(copies)]
    for copy in copies:
        copy.start()
    copies[0].wait()
    copies[1].wait()
    inverse = turn_ref[:1]
    groups = TOK // 8
    angles = (rank * TOK + 8 * rows_of((groups, 128))).astype(f32) * inverse
    coarse_ref[0] = jnp.cos(angles)
    coarse_ref[1] = jnp.sin(angles)
    angles = rows_of((8, 128)).astype(f32) * inverse
    fine_cos = jnp.cos(angles)
    fine_sin = jnp.sin(angles)
    for group in range(groups):
        cosine = coarse_ref[0, group : group + 1, :]
        sine = coarse_ref[1, group : group + 1, :]
        rows = slice(8 * group, 8 * group + 8)
        cos_ref[rows, :] = cosine * fine_cos - sine * fine_sin
        sin_ref[rows, :] = (sine * fine_cos + cosine * fine_sin) * turn_ref[1:]
    chosen = chosen_ref[...]
    query_block = rank * QB + rows_of(chosen.shape)
    wanted = jnp.where((chosen <= query_block) & (chosen // QB != rank), chosen, -1)
    every = lanes_of((QB, NBLK))
    hit = jnp.zeros((QB, NBLK), f32)
    for k in range(NSEL):
        hit = jnp.where(every == wanted[:, k : k + 1], 1.0, hit)
    present = jnp.broadcast_to(jnp.max(hit, 0, keepdims=True), (8, NBLK))
    lane = lanes_of((8, NBLK))
    running = present
    for step in (1, 2, 4, 8):
        running = running + jnp.where(lane % QB >= step, pltpu.roll(running, step, 1), 0.0)
    code_ref[...] = jnp.where(present > 0.0, running - present, UNUSED)
    for copy in copies[2:6]:
        copy.wait()
    for c in range(CHUNKS):
        copies[6 + c].wait()
        rows = slice(c * part, c * part + part)
        four = dot_t(tokens_ref[rows], weight_ref[...])
        raw_ref[rows] = four[:, :128].astype(bf16).astype(f32)
        pair = four[:, 128:]
        lane = lanes_of(pair.shape)
        pair = jnp.where(lane < HD, turned(pair, cos_ref[rows, :], sin_ref[rows, :]), pair).astype(bf16)
        payload_ref[rows, :] = pair
    for copy in copies[6 + CHUNKS :]:
        copy.wait()
    ends = (rank * NSUM + rows_of((NSUM, 128))) * CMP_STRIDE + 2 * CMP_STRIDE - 1
    cosine, sine = turns(ends, turn_ref)
    zero = jnp.zeros((HD, 128), bf16)
    total = jnp.zeros((NSUM, 512), f32)
    for p in range(0, CMP_STRIDE, 2):
        left = []
        right = []
        for q in (p, p + 1):
            left.append(raw_ref[pl.ds(q, NSUM, stride=CMP_STRIDE), :].astype(bf16))
            low = pl.ds(q * HD, HD)
            high = pl.ds((q + CMP_STRIDE) * HD, HD)
            right.append(jnp.concatenate([ink_ref[low, :], ink_ref[high, :], zero, zero], 1))
            right.append(jnp.concatenate([zero, zero, inv_ref[low, :], inv_ref[high, :]], 1))
        total = total + dot(jnp.concatenate(left, 1), jnp.concatenate(right, 0))
    low_k, high_k = total[:, :128], total[:, 128:256]
    low_v, high_v = total[:, 256:384], total[:, 384:]
    pre_k = low_k + pltpu.roll(high_k, NSUM - 1, 0)
    pre_v = low_v + pltpu.roll(high_v, NSUM - 1, 0)
    summaries = squeeze_out(pre_k, pre_v, outk_ref[...], outv_ref[...], cosine, sine)
    edges = [low_k[NSUM - 1 :], low_v[NSUM - 1 :], high_k[:1], high_v[:1]]
    rest = jnp.zeros((ROWS - NSUM - 4, 128), f32)
    extra = jnp.concatenate([summaries, *edges, rest], 0).astype(bf16)
    payload_ref[TOK:, :] = extra


def query_kernel(
    tokens_ref, wq_ref, gate_ref, cos_ref, sin_ref, chosen_ref, code_ref,
    query_ref, gates_ref, place_ref, bound_ref,
):
    @pl.when(pl.program_id(0) == 0)
    def _():
        rank = kv_index()
        chosen = chosen_ref[...]
        query_block = rank * QB + rows_of(chosen.shape)
        code = code_ref[...]
        code = jnp.concatenate([code, code], 0)
        every = lanes_of((QB, NBLK))
        slot_lane = lanes_of((QB, NSEL))
        slot = jnp.zeros((QB, NSEL), f32)
        for k in range(NSEL):
            found = jnp.where(every == chosen[:, k : k + 1], code, 0.0)
            slot = jnp.where(slot_lane == k, jnp.sum(found, 1, keepdims=True), slot)
        holder = chosen // QB
        arrival = holder % COLUMNS * LAYERS + holder // COLUMNS
        place = jnp.where(
            holder == rank, PEERS * CAP + chosen % QB, arrival * CAP + slot.astype(jnp.int32)
        )
        place_ref[...] = jnp.where(chosen <= query_block, place, PEERS * CAP)
        order = jnp.where(chosen < query_block, -1.0, jnp.where(chosen > query_block, 1.0, 0.0))
        spread = (lanes_of((NSEL, NSEL * BLK)) // BLK == rows_of((NSEL, NSEL * BLK))).astype(bf16)
        inner = (lanes_of((QB, NSEL * BLK)) % BLK).astype(f32)
        bound_ref[...] = dot(order.astype(bf16), spread) * 64.0 + inner

    cosine = cos_ref[...]
    sine = sin_ref[...]
    lane = lanes_of(cosine.shape)
    gate = jnp.concatenate([gate_ref[0], gate_ref[1]], 0)
    gates_ref[...] = jax.nn.sigmoid(dot_t(tokens_ref[...], gate))
    queries = dot(tokens_ref[...], wq_ref[...]) * np.float32(HD ** -0.5)
    for side in range(2):
        both = turned(queries[:, 128 * side : 128 * side + 128], cosine, sine)
        for half in range(2):
            head = 2 * side + half
            one = both if half == 0 else pltpu.roll(both, HD, 1)
            one = jnp.where(lane < HD, one, 0.0).astype(bf16)
            for b in range(PART // BLK):
                query_ref[b, head * BLK : (head + 1) * BLK, :] = one[b * BLK : (b + 1) * BLK]


def pick_kernel(
    code0_ref, code1_ref, code2_ref, code3_ref, own_ref, up1_ref, up2_ref, up3_ref, far_a_ref,
    far_b_ref, down3_ref, down2_ref, down1_ref, picked_ref, column_ref,
    far_ref, code_ref, ids_ref, ids_smem, sem,
):
    asker = pl.program_id(0)
    place = lax.axis_index("z")
    stock = (own_ref, up1_ref, up2_ref, up3_ref, far_ref, down3_ref, down2_ref, down1_ref)

    @pl.when(asker == 0)
    def _():
        column = lax.axis_index("x")
        for d, ref in enumerate((code0_ref, code1_ref, code2_ref, code3_ref)):
            code_ref[(column - d + COLUMNS) % COLUMNS] = ref[...]
        lane = lanes_of((LAYERS, NBLK))
        mine = lane // QB == rows_of((LAYERS, NBLK)) * COLUMNS + column
        inner = (lane % QB).astype(f32)
        spot = lanes_of((LAYERS, 128))
        for n in range(COLUMNS):
            code = code_ref[n]
            ids = jnp.zeros((LAYERS, 128), f32)
            for s in range(CAP):
                value = jnp.sum(jnp.where(mine & (code == float(s)), inner, 0.0), 1, keepdims=True)
                ids = jnp.where(spot == s, value, ids)
            ids_ref[n * LAYERS : (n + 1) * LAYERS, :] = ids.astype(jnp.int32)
        copy = pltpu.make_async_copy(ids_ref, ids_smem, sem)
        copy.start()
        far_ref[:SPLIT, :] = far_a_ref[...]
        far_ref[SPLIT:, :] = far_b_ref[...]
        for d, ref in enumerate(stock):
            column_ref[(place - d + LAYERS) % LAYERS] = ref[TOK:, :]
        copy.wait()

    for d, ref in enumerate(stock):
        layer = (place - d + LAYERS) % LAYERS
        for s in range(CAP):
            start = pl.multiple_of(ids_smem[asker * LAYERS + layer, s] * BLK, BLK)
            row = pl.multiple_of((layer * CAP + s) * BLK, BLK)
            picked_ref[0, pl.ds(row, BLK), :] = ref[pl.ds(start, BLK), :]


def mixed_heads(result, gates, first):
    lane = lanes_of((BLK, 128))
    halves = []
    for pair in range(2):
        gated = []
        for head in (2 * pair, 2 * pair + 1):
            gate = gates[:, first + head : first + head + 1]
            gated.append(result[head * BLK : (head + 1) * BLK] * gate)
        halves.append(jnp.where(lane < HD, pltpu.roll(gated[0], HD, 1), gated[1]))
    return halves


def compressed_kernel(
    column0_ref, column1_ref, column2_ref, column3_ref, query_ref, gates_ref, outk_ref, outv_ref,
    turn_ref, mixed_ref, arrived_ref, key_ref, value_ref, score_ref, weight_ref,
):
    rank = kv_index()
    column = lax.axis_index("x")
    for d, ref in enumerate((column0_ref, column1_ref, column2_ref, column3_ref)):
        arrived_ref[(column - d + COLUMNS) % COLUMNS] = ref[...]
    flat = arrived_ref[...].reshape(PEERS * ROWS, 128)
    shape = (4 * PEERS, PEERS * ROWS)
    row = rows_of(shape)
    kind = row // PEERS
    source = row % PEERS + kind % 2
    target = (source % COLUMNS * LAYERS + source // COLUMNS) * ROWS + NSUM + jnp.where(kind == 0, 0, jnp.where(kind == 1, 2, jnp.where(kind == 2, 1, 3)))
    edges = dot(((lanes_of(shape) == target) & (source < PEERS)).astype(bf16), flat)
    pre_k = edges[:PEERS] + edges[PEERS : 2 * PEERS]
    pre_v = edges[2 * PEERS : 3 * PEERS] + edges[3 * PEERS :]
    ends = rows_of((PEERS, 128)) * TOK + TOK + CMP_STRIDE - 1
    last = squeeze_out(pre_k, pre_v, outk_ref[...], outv_ref[...], *turns(ends, turn_ref))
    is_last = rows_of((NSUM, 128)) == NSUM - 1
    lane = lanes_of((NSUM, 128))
    for peer in range(PEERS):
        chunk = arrived_ref[peer % COLUMNS, peer // COLUMNS, :NSUM, :].astype(f32)
        chunk = jnp.where(is_last, last[peer : peer + 1], chunk)
        value_ref[peer * NSUM : (peer + 1) * NSUM, :] = jnp.where(lane < HD, 1.0, chunk).astype(bf16)
        key_ref[peer * NSUM : (peer + 1) * NSUM, :] = chunk.astype(bf16)
    group = COMPRESSED * HEADS * BLK
    columns = lanes_of((HEADS * BLK, PEERS * NSUM))
    inside = lax.broadcasted_iota(jnp.int32, (HEADS * BLK, 1), 0) % BLK

    def score(step, carry):
        rows = query_ref[pl.ds(step * COMPRESSED, COMPRESSED)].reshape(group, 128)
        score_ref[pl.ds(pl.multiple_of(step * group, group), group), :] = dot_t(rows, key_ref[...])
        return carry

    def weigh(step, carry):
        for j in range(COMPRESSED):
            b = step * COMPRESSED + j
            rows = pl.ds(pl.multiple_of(b * HEADS * BLK, HEADS * BLK), HEADS * BLK)
            limit = (rank * TOK + b * BLK + inside - (2 * CMP_STRIDE - 1)) >> 4
            scores = jnp.where(columns <= limit, score_ref[rows, :], NEG)
            largest = jnp.maximum(jnp.max(scores, 1, keepdims=True), FLOOR)
            weight_ref[rows, :] = jnp.exp(scores - largest).astype(bf16)
        return carry

    def mix(step, carry):
        rows = pl.ds(pl.multiple_of(step * group, group), group)
        result = dot(weight_ref[rows, :], value_ref[...])
        result = result / jnp.maximum(pltpu.roll(result, HD, 1), 1.0)
        for j in range(COMPRESSED):
            start = pl.multiple_of((step * COMPRESSED + j) * BLK, BLK)
            one = result[j * HEADS * BLK : (j + 1) * HEADS * BLK]
            halves = mixed_heads(one, gates_ref[pl.ds(start, BLK), :], 0)
            mixed_ref[pl.ds(start, BLK), :128] = halves[0].astype(bf16)
            mixed_ref[pl.ds(start, BLK), 128:] = halves[1].astype(bf16)
        return carry

    lax.fori_loop(0, QB // COMPRESSED, score, 0)
    lax.fori_loop(0, QB // COMPRESSED, weigh, 0)
    lax.fori_loop(0, QB // COMPRESSED, mix, 0)


def selected_kernel(
    place_hbm, fetched_hbm, pair_hbm, query_hbm, bound_hbm, gates_hbm, mixed_hbm,
    out0_ref, out1_ref, out2_ref, out3_ref,
    place_ref, fetched_ref, pair_ref, query_ref, bound_ref, gates_ref, mixed_ref,
    key_ref, score_ref, weight_ref, out_ref, sems,
):
    chip = lax.axis_index("tp") // 2
    copies = [
        (place_hbm, place_ref),
        (fetched_hbm, fetched_ref),
        (pair_hbm.at[pl.ds(0, TOK)], pair_ref),
        (query_hbm, query_ref),
        (bound_hbm, bound_ref),
        (gates_hbm, gates_ref),
        (mixed_hbm, mixed_ref),
    ]
    copies = [pltpu.make_async_copy(a, b, sems.at[n]) for n, (a, b) in enumerate(copies)]
    for copy in copies:
        copy.start()
    inside = (lax.broadcasted_iota(jnp.int32, (HEADS * BLK, 1), 0) % BLK).astype(f32)
    lane = lanes_of((NSEL * BLK, 128))

    def score(step, carry):
        for j in range(GATHERED):
            b = step * GATHERED + j
            for k in range(NSEL):
                place = place_ref[b, k]
                far_row = pl.multiple_of(jnp.minimum(place, PEERS * CAP - 1) * BLK, BLK)
                near_row = pl.multiple_of(jnp.maximum(place - PEERS * CAP, 0) * BLK, BLK)
                is_near = jnp.full((BLK, 128), place, jnp.int32) >= PEERS * CAP
                key_ref[b, k * BLK : (k + 1) * BLK, :] = jnp.where(
                    is_near, pair_ref[pl.ds(near_row, BLK), :], fetched_ref[pl.ds(far_row, BLK), :]
                )
            score_ref[b] = dot_t(query_ref[b], key_ref[b])
        return carry

    def weigh(step, carry):
        for j in range(WEIGHED):
            b = step * WEIGHED + j
            scores = jnp.where(bound_ref[pl.ds(b, 1), :] <= inside, score_ref[b], NEG)
            largest = jnp.max(scores, 1, keepdims=True)
            weight_ref[b] = jnp.exp(scores - largest).astype(bf16)
        return carry

    def mix(step, carry):
        for j in range(MIXED):
            b = step * MIXED + j
            keys = key_ref[b]
            values = jnp.where(lane < HD, jnp.ones_like(keys), keys)
            result = dot(weight_ref[b], values)
            result = result / pltpu.roll(result, HD, 1)
            start = pl.multiple_of(b * BLK, BLK)
            halves = mixed_heads(result, gates_ref[pl.ds(start, BLK), :], HEADS)
            row = pl.multiple_of((b % PER_CHIP) * BLK, BLK)
            for side in range(2):
                cols = slice(128 * side, 128 * side + 128)
                out_ref[(b // PER_CHIP - chip + CHIPS) % CHIPS, pl.ds(row, BLK), cols] = (
                    mixed_ref[pl.ds(start, BLK), cols] + halves[side]
                ).astype(bf16)
        return carry

    for copy in copies[:4]:
        copy.wait()
    lax.fori_loop(0, QB // GATHERED, score, 0)
    copies[4].wait()
    lax.fori_loop(0, QB // WEIGHED, weigh, 0)
    copies[5].wait()
    copies[6].wait()
    lax.fori_loop(0, QB // MIXED, mix, 0)
    for d, ref in enumerate((out0_ref, out1_ref, out2_ref, out3_ref)):
        ref[...] = out_ref[d]


def output_kernel(
    a0_ref, a1_ref, a2_ref, a3_ref, w0_ref, w1_ref, w2_ref, w3_ref,
    mine_ref, other_ref, sum_ref,
):
    core = lax.axis_index("tp") % 2
    total = dot(a0_ref[...], w0_ref[...])
    total = total + dot(a1_ref[...], w1_ref[...])
    total = total + dot(a3_ref[...], w3_ref[...])
    total = total + dot(a2_ref[...], w2_ref[...])
    sum_ref[...] = total
    mine_ref[...] = sum_ref[pl.ds(pl.multiple_of(core * OUT_ROWS, OUT_ROWS), OUT_ROWS), :]
    other = pl.multiple_of((1 - core) * OUT_ROWS, OUT_ROWS)
    other_ref[...] = sum_ref[pl.ds(other, OUT_ROWS), :].astype(bf16)


VMEM = pl.BlockSpec(memory_space=pltpu.VMEM)
SMEM = pl.BlockSpec(memory_space=pltpu.SMEM)
HBM = pl.BlockSpec(memory_space=pltpu.HBM)


def shape_of(shape, dtype):
    return jax.ShapeDtypeStruct(shape, dtype)


def stored(shape, dtype):
    return pltpu.HBM(shape, dtype)


def far(*values):
    return [pltpu.with_memory_space_constraint(value, pltpu.HBM) for value in values]


def limit(mib):
    return pltpu.CompilerParams(vmem_limit_bytes=mib * 1024 * 1024)


def across(value, distance):
    return lax.ppermute(value, "z", [(i, (i + distance) % LAYERS) for i in range(LAYERS)])


def along(value, distance):
    return lax.ppermute(value, "x", [(i, (i + distance) % COLUMNS) for i in range(COLUMNS)])


def around(value, distance):
    route = [(2 * y + c, 2 * ((y + distance) % CHIPS) + c) for y in range(CHIPS) for c in range(2)]
    return lax.ppermute(value, "tp", route)


def on_device(
    tokens, query_weight, chosen_key_weight, chosen_value_weight, summary_key_weight,
    summary_value_weight, squeeze_key_in, squeeze_key_out, squeeze_value_in, squeeze_value_out,
    gate_weight, output_weight, chosen_blocks,
):
    chosen = chosen_blocks[0]
    squeeze_key_t = squeeze_key_out.T
    squeeze_value_t = squeeze_value_out.T
    turn = jnp.asarray(np.concatenate([INVERSE_ROW, SIGN_ROW], 0))
    row_block = pl.BlockSpec((PART, 128), lambda n: (n, 0))
    token_block = pl.BlockSpec((PART, 2048), lambda n: (n, 0))
    payload, code, cosine, sine = pl.pallas_call(
        token_kernel,
        name="tokens",
        out_shape=(
            stored((TOK + ROWS, 128), bf16),
            stored((8, NBLK), f32),
            stored((TOK, 128), f32),
            stored((TOK, 128), f32),
        ),
        in_specs=[HBM] * 11,
        out_specs=(VMEM,) * 4,
        scratch_shapes=[
            pltpu.VMEM((TOK, 2048), bf16),
            pltpu.VMEM((4 * HD, 2048), bf16),
            pltpu.VMEM((2048, 128), bf16),
            pltpu.VMEM((2048, 128), bf16),
            pltpu.VMEM((HD, 128), bf16),
            pltpu.VMEM((HD, 128), bf16),
            pltpu.VMEM((2, 128), f32),
            pltpu.VMEM((QB, NSEL), jnp.int32),
            pltpu.VMEM((TOK, 128), f32),
            pltpu.VMEM((2, TOK // 8, 128), f32),
            pltpu.SemaphoreType.DMA((10 + CHUNKS,)),
        ],
        compiler_params=limit(24),
        cost_estimate=pl.CostEstimate(flops=10**9, bytes_accessed=5 * 10**6, transcendentals=0),
    )(
        *far(
            tokens, summary_key_weight.T, summary_value_weight.T, chosen_key_weight.T,
            chosen_value_weight.T, squeeze_key_in, squeeze_value_in, squeeze_key_t, squeeze_value_t,
            turn, chosen,
        ),
    )
    up2 = across(payload, 2)
    down2 = across(payload, -2)
    up1 = across(payload, 1)
    down1 = across(payload, -1)
    codes = [code] + [along(code, d) for d in range(1, COLUMNS)]
    weight_1 = around(output_weight, 1)
    weight_3 = around(output_weight, -1)
    far_a = across(up2[:SPLIT], 2)
    far_b = across(down2[SPLIT:], -2)
    up3 = across(up2, 1)
    down3 = across(down2, -1)
    queries, gates, place, bound = pl.pallas_call(
        query_kernel,
        name="queries",
        out_shape=(
            stored((QB, HEADS * BLK, 128), bf16),
            stored((TOK, 2 * HEADS), f32),
            stored((QB, NSEL), jnp.int32),
            stored((QB, NSEL * BLK), f32),
        ),
        grid=(TOK // PART,),
        in_specs=[
            token_block, VMEM, VMEM, row_block, row_block, VMEM, VMEM,
        ],
        out_specs=(
            pl.BlockSpec((PART // BLK, HEADS * BLK, 128), lambda n: (n, 0, 0)),
            pl.BlockSpec((PART, 2 * HEADS), lambda n: (n, 0)),
            VMEM,
            VMEM,
        ),
        compiler_params=limit(16),
        cost_estimate=pl.CostEstimate(flops=10**10, bytes_accessed=3 * 10**6, transcendentals=0),
    )(*far(tokens, query_weight), gate_weight.transpose(0, 2, 1), *far(cosine, sine, chosen, code))
    picked, column = pl.pallas_call(
        pick_kernel,
        name="pick",
        out_shape=(
            stored((COLUMNS, LAYERS * CAP * BLK, 128), bf16),
            stored((LAYERS, ROWS, 128), bf16),
        ),
        grid=(COLUMNS,),
        in_specs=[VMEM] * (COLUMNS + 9),
        out_specs=(pl.BlockSpec((1, LAYERS * CAP * BLK, 128), lambda n: (n, 0, 0)), VMEM),
        scratch_shapes=[
            pltpu.VMEM((TOK + ROWS, 128), bf16),
            pltpu.VMEM((COLUMNS, 8, NBLK), f32),
            pltpu.VMEM((PEERS, 128), jnp.int32),
            pltpu.SMEM((PEERS, 128), jnp.int32),
            pltpu.SemaphoreType.DMA,
        ],
        compiler_params=limit(8),
    )(*far(code), *codes[1:], *far(payload), up1, up2, up3, far_a, far_b, down3, down2, down1)
    fetched = lax.all_to_all(picked, "x", 0, 0, tiled=True)
    columns = [column] + [along(column, d) for d in range(1, COLUMNS)]
    weight_2 = around(weight_1, 1)
    mixed = pl.pallas_call(
        compressed_kernel,
        name="compressed",
        out_shape=stored((TOK, HEADS * HD), bf16),
        in_specs=[VMEM] * (COLUMNS + 5),
        out_specs=VMEM,
        scratch_shapes=[
            pltpu.VMEM((COLUMNS, LAYERS, ROWS, 128), bf16),
            pltpu.VMEM((PEERS * NSUM, 128), bf16),
            pltpu.VMEM((PEERS * NSUM, 128), bf16),
            pltpu.VMEM((QB * HEADS * BLK, PEERS * NSUM), f32),
            pltpu.VMEM((QB * HEADS * BLK, PEERS * NSUM), bf16),
        ],
        compiler_params=limit(24),
        cost_estimate=pl.CostEstimate(flops=10**10, bytes_accessed=3 * 10**6, transcendentals=0),
    )(*columns, *far(queries, gates, squeeze_key_t, squeeze_value_t, turn))
    pieces = pl.pallas_call(
        selected_kernel,
        name="selected",
        out_shape=(shape_of((PER_CHIP * BLK, HEADS * HD), bf16),) * CHIPS,
        in_specs=[HBM] * 7,
        out_specs=(VMEM,) * CHIPS,
        scratch_shapes=[
            pltpu.SMEM((QB, NSEL), jnp.int32),
            pltpu.VMEM((PEERS * CAP * BLK, 128), bf16),
            pltpu.VMEM((TOK, 128), bf16),
            pltpu.VMEM((QB, HEADS * BLK, 128), bf16),
            pltpu.VMEM((QB, NSEL * BLK), f32),
            pltpu.VMEM((TOK, 2 * HEADS), f32),
            pltpu.VMEM((TOK, HEADS * HD), bf16),
            pltpu.VMEM((QB, NSEL * BLK, 128), bf16),
            pltpu.VMEM((QB, HEADS * BLK, NSEL * BLK), f32),
            pltpu.VMEM((QB, HEADS * BLK, NSEL * BLK), bf16),
            pltpu.VMEM((CHIPS, PER_CHIP * BLK, HEADS * HD), bf16),
            pltpu.SemaphoreType.DMA((7,)),
        ],
        compiler_params=limit(24),
        cost_estimate=pl.CostEstimate(flops=10**9, bytes_accessed=3 * 10**6, transcendentals=0),
    )(
        *far(place, fetched.reshape(PEERS * CAP * BLK, 128), payload, queries, bound, gates, mixed),
    )
    piece_2 = around(pieces[2], 2)
    piece_1 = around(pieces[1], 1)
    piece_3 = around(pieces[3], -1)
    mine, other = pl.pallas_call(
        output_kernel,
        name="output",
        out_shape=(shape_of((OUT_ROWS, 2048), f32), shape_of((OUT_ROWS, 2048), bf16)),
        in_specs=[VMEM] * 8,
        out_specs=(VMEM, VMEM),
        scratch_shapes=[pltpu.VMEM((2 * OUT_ROWS, 2048), f32)],
        compiler_params=limit(16),
    )(
        pieces[0], piece_1, piece_2, piece_3, output_weight, weight_1, weight_2, weight_3,
    )
    swapped = lax.ppermute(other, "tp", [(i, i ^ 1) for i in range(2 * CHIPS)])
    return (mine + swapped.astype(f32)).astype(bf16)


def solution(mesh):
    split = Mesh(mesh.devices.reshape(LAYERS, COLUMNS, 2 * CHIPS), ("z", "x", "tp"))
    kv = ("z", "x")
    return jax.shard_map(
        on_device,
        mesh=split,
        in_specs=(
            P(kv, None),
            P(None, "tp"),
            P(None, "tp"),
            P(None, "tp"),
            P(None, "tp"),
            P(None, "tp"),
            P(),
            P(),
            P(),
            P(),
            P(None, None, "tp"),
            P("tp", None),
            P("tp", kv, None),
        ),
        out_specs=P(("z", "x", "tp"), None),
        check_vma=False,
    )
```

```python
import jax
import jax.numpy as jnp
import numpy as np
from jax import lax
from jax.experimental import pallas as pl
from jax.experimental.pallas import tpu as pltpu
from jax.sharding import Mesh
from jax.sharding import PartitionSpec as P


HD = 64
CMP_STRIDE = 16
BLK = 32
NSEL = 16
CAP = 4
ROTARY_BASE = 10000.0
NEG = -1e30
FLOOR = -1e29
TOK = 512
PEERS = 32
LAYERS = 8
COLUMNS = 4
NSUM = 32
ROWS = 40
QB = TOK // BLK
HEADS = 4
NBLK = PEERS * QB
UNUSED = 99.0
COMPRESSED = 4
CHIPS = 4
PER_CHIP = QB // CHIPS
CHUNKS = 2
SPLIT = 288
GATHERED = 16
WEIGHED = 4
MIXED = 8
OUT_ROWS = TOK // 8

INVERSE = (ROTARY_BASE ** (-np.arange(HD // 2, dtype=np.float64) / (HD // 2))).astype(np.float32)
INVERSE_ROW = np.tile(INVERSE, 4)[None, :]
SIGN_ROW = np.tile(np.repeat(np.array([-1.0, 1.0], np.float32), HD // 2), 2)[None, :]

bf16 = jnp.bfloat16
f32 = jnp.float32


def kv_index():
    return lax.axis_index("z") * COLUMNS + lax.axis_index("x")


def dot(a, b):
    return jnp.dot(a, b, preferred_element_type=f32)


def dot_t(a, b):
    return lax.dot_general(a, b, (((1,), (1,)), ((), ())), preferred_element_type=f32)


def lanes_of(shape):
    return lax.broadcasted_iota(jnp.int32, shape, len(shape) - 1)


def rows_of(shape):
    return lax.broadcasted_iota(jnp.int32, shape, len(shape) - 2)


def turned(x, cosine, sine):
    lane = lanes_of(x.shape)
    swapped = jnp.where(lane % HD < HD // 2, pltpu.roll(x, 128 - HD // 2, 1), pltpu.roll(x, HD // 2, 1))
    return x * cosine + swapped * sine


def turns(positions, turn_ref):
    angles = positions.astype(f32) * turn_ref[:1]
    return jnp.cos(angles), jnp.sin(angles) * turn_ref[1:]


def gelu(x):
    return 0.5 * x * (1.0 + jnp.tanh(np.float32(np.sqrt(2.0 / np.pi)) * (x + 0.044715 * (x * x * x))))


def squeeze_out(pre_k, pre_v, out_k, out_v, cosine, sine):
    hidden = jnp.concatenate([gelu(pre_k).astype(bf16), gelu(pre_v).astype(bf16)], 1)
    zero = jnp.zeros(out_k.shape, bf16)
    weight = jnp.concatenate(
        [jnp.concatenate([out_k, zero], 1), jnp.concatenate([zero, out_v], 1)], 0
    )
    both = dot_t(hidden, weight)
    return jnp.where(lanes_of(both.shape) < HD, turned(both, cosine, sine), both)


def token_kernel(
    tokens_hbm, wk_hbm, wv_hbm, ck_hbm, cv_hbm, ink_hbm, inv_hbm, outk_hbm, outv_hbm, turn_hbm,
    chosen_hbm, payload_ref, code_ref, cos_ref, sin_ref, place_ref, bound_ref,
    tokens_ref, weight_ref, ink_ref, inv_ref, outk_ref, outv_ref, turn_ref, chosen_ref, raw_ref,
    coarse_ref, sems,
):
    rank = kv_index()
    part = TOK // CHUNKS
    copies = [
        (chosen_hbm, chosen_ref),
        (turn_hbm, turn_ref),
        (wk_hbm, weight_ref.at[:HD]),
        (wv_hbm, weight_ref.at[HD : 2 * HD]),
        (ck_hbm, weight_ref.at[2 * HD : 3 * HD]),
        (cv_hbm, weight_ref.at[3 * HD :]),
        *((tokens_hbm.at[pl.ds(c * part, part)], tokens_ref.at[pl.ds(c * part, part)]) for c in range(CHUNKS)),
        (ink_hbm, ink_ref),
        (inv_hbm, inv_ref),
        (outk_hbm, outk_ref),
        (outv_hbm, outv_ref),
    ]
    copies = [pltpu.make_async_copy(a, b, sems.at[n]) for n, (a, b) in enumerate(copies)]
    for copy in copies:
        copy.start()
    copies[0].wait()
    copies[1].wait()
    inverse = turn_ref[:1]
    groups = TOK // 8
    angles = (rank * TOK + 8 * rows_of((groups, 128))).astype(f32) * inverse
    coarse_ref[0] = jnp.cos(angles)
    coarse_ref[1] = jnp.sin(angles)
    angles = rows_of((8, 128)).astype(f32) * inverse
    fine_cos = jnp.cos(angles)
    fine_sin = jnp.sin(angles)
    for group in range(groups):
        cosine = coarse_ref[0, group : group + 1, :]
        sine = coarse_ref[1, group : group + 1, :]
        rows = slice(8 * group, 8 * group + 8)
        cos_ref[rows, :] = cosine * fine_cos - sine * fine_sin
        sin_ref[rows, :] = (sine * fine_cos + cosine * fine_sin) * turn_ref[1:]
    chosen = chosen_ref[...]
    query_block = rank * QB + rows_of(chosen.shape)
    wanted = jnp.where((chosen <= query_block) & (chosen // QB != rank), chosen, -1)
    every = lanes_of((QB, NBLK))
    hit = jnp.zeros((QB, NBLK), f32)
    for k in range(NSEL):
        hit = jnp.where(every == wanted[:, k : k + 1], 1.0, hit)
    present = jnp.broadcast_to(jnp.max(hit, 0, keepdims=True), (8, NBLK))
    lane = lanes_of((8, NBLK))
    running = present
    for step in (1, 2, 4, 8):
        running = running + jnp.where(lane % QB >= step, pltpu.roll(running, step, 1), 0.0)
    code = jnp.where(present > 0.0, running - present, UNUSED)
    code_ref[...] = code
    code = jnp.concatenate([code, code], 0)
    slot_lane = lanes_of((QB, NSEL))
    slot = jnp.zeros((QB, NSEL), f32)
    for k in range(NSEL):
        found = jnp.where(every == chosen[:, k : k + 1], code, 0.0)
        slot = jnp.where(slot_lane == k, jnp.sum(found, 1, keepdims=True), slot)
    holder = chosen // QB
    arrival = holder % COLUMNS * LAYERS + holder // COLUMNS
    place = jnp.where(
        holder == rank, PEERS * CAP + chosen % QB, arrival * CAP + slot.astype(jnp.int32)
    )
    place_ref[...] = jnp.where(chosen <= query_block, place, PEERS * CAP)
    order = jnp.where(chosen < query_block, -1.0, jnp.where(chosen > query_block, 1.0, 0.0))
    spread = (lanes_of((NSEL, NSEL * BLK)) // BLK == rows_of((NSEL, NSEL * BLK))).astype(bf16)
    inner = (lanes_of((QB, NSEL * BLK)) % BLK).astype(f32)
    bound_ref[...] = dot(order.astype(bf16), spread) * 64.0 + inner
    for copy in copies[2:6]:
        copy.wait()
    for c in range(CHUNKS):
        copies[6 + c].wait()
        rows = slice(c * part, c * part + part)
        four = dot_t(tokens_ref[rows], weight_ref[...])
        raw_ref[rows] = four[:, :128].astype(bf16).astype(f32)
        pair = four[:, 128:]
        lane = lanes_of(pair.shape)
        pair = jnp.where(lane < HD, turned(pair, cos_ref[rows, :], sin_ref[rows, :]), pair).astype(bf16)
        payload_ref[rows, :] = pair
    for copy in copies[6 + CHUNKS :]:
        copy.wait()
    ends = (rank * NSUM + rows_of((NSUM, 128))) * CMP_STRIDE + 2 * CMP_STRIDE - 1
    cosine, sine = turns(ends, turn_ref)
    zero = jnp.zeros((HD, 128), bf16)
    total = jnp.zeros((NSUM, 512), f32)
    for p in range(0, CMP_STRIDE, 2):
        left = []
        right = []
        for q in (p, p + 1):
            left.append(raw_ref[pl.ds(q, NSUM, stride=CMP_STRIDE), :].astype(bf16))
            low = pl.ds(q * HD, HD)
            high = pl.ds((q + CMP_STRIDE) * HD, HD)
            right.append(jnp.concatenate([ink_ref[low, :], ink_ref[high, :], zero, zero], 1))
            right.append(jnp.concatenate([zero, zero, inv_ref[low, :], inv_ref[high, :]], 1))
        total = total + dot(jnp.concatenate(left, 1), jnp.concatenate(right, 0))
    low_k, high_k = total[:, :128], total[:, 128:256]
    low_v, high_v = total[:, 256:384], total[:, 384:]
    pre_k = low_k + pltpu.roll(high_k, NSUM - 1, 0)
    pre_v = low_v + pltpu.roll(high_v, NSUM - 1, 0)
    summaries = squeeze_out(pre_k, pre_v, outk_ref[...], outv_ref[...], cosine, sine)
    edges = [low_k[NSUM - 1 :], low_v[NSUM - 1 :], high_k[:1], high_v[:1]]
    rest = jnp.zeros((ROWS - NSUM - 4, 128), f32)
    extra = jnp.concatenate([summaries, *edges, rest], 0).astype(bf16)
    payload_ref[TOK:, :] = extra


def query_kernel(
    tokens_ref, wq_ref, gate_ref, cos_ref, sin_ref, code0_ref, code1_ref, code2_ref, code3_ref,
    query_ref, gates_ref, ids_ref, code_ref,
):
    column = lax.axis_index("x")
    for d, ref in enumerate((code0_ref, code1_ref, code2_ref, code3_ref)):
        code_ref[(column - d + COLUMNS) % COLUMNS] = ref[...]
    every = lanes_of((LAYERS, NBLK))
    mine = every // QB == rows_of((LAYERS, NBLK)) * COLUMNS + column
    inner = (every % QB).astype(f32)
    spot = lanes_of((LAYERS, 128))
    for n in range(COLUMNS):
        code = code_ref[n]
        ids = jnp.zeros((LAYERS, 128), f32)
        for s in range(CAP):
            value = jnp.sum(jnp.where(mine & (code == float(s)), inner, 0.0), 1, keepdims=True)
            ids = jnp.where(spot == s, value, ids)
        ids_ref[n * LAYERS : (n + 1) * LAYERS, :] = ids.astype(jnp.int32)
    cosine = cos_ref[...]
    sine = sin_ref[...]
    lane = lanes_of(cosine.shape)
    gate = jnp.concatenate([gate_ref[0], gate_ref[1]], 0)
    gates_ref[...] = jax.nn.sigmoid(dot_t(tokens_ref[...], gate))
    queries = dot(tokens_ref[...], wq_ref[...]) * np.float32(HD ** -0.5)
    for side in range(2):
        both = turned(queries[:, 128 * side : 128 * side + 128], cosine, sine)
        for half in range(2):
            head = 2 * side + half
            one = both if half == 0 else pltpu.roll(both, HD, 1)
            one = jnp.where(lane < HD, one, 0.0).astype(bf16)
            for b in range(QB):
                query_ref[b, head * BLK : (head + 1) * BLK, :] = one[b * BLK : (b + 1) * BLK]


def pick_kernel(
    ids_hbm, own_hbm, up1_ref, up2_ref, up3_ref, far_a_ref, far_b_ref, down3_ref, down2_ref,
    down1_ref, picked_ref, column_ref, own_ref, far_ref, ids_smem, sems,
):
    asker = pl.program_id(0)
    place = lax.axis_index("z")
    stock = (own_ref, up1_ref, up2_ref, up3_ref, far_ref, down3_ref, down2_ref, down1_ref)

    @pl.when(asker == 0)
    def _():
        copies = [
            pltpu.make_async_copy(own_hbm, own_ref, sems.at[0]),
            pltpu.make_async_copy(ids_hbm, ids_smem, sems.at[1]),
        ]
        for copy in copies:
            copy.start()
        far_ref[:SPLIT, :] = far_a_ref[...]
        far_ref[SPLIT:, :] = far_b_ref[...]
        for copy in copies:
            copy.wait()
        for d, ref in enumerate(stock):
            column_ref[(place - d + LAYERS) % LAYERS] = ref[TOK:, :]

    for d, ref in enumerate(stock):
        layer = (place - d + LAYERS) % LAYERS
        for s in range(CAP):
            start = pl.multiple_of(ids_smem[asker * LAYERS + layer, s] * BLK, BLK)
            row = pl.multiple_of((layer * CAP + s) * BLK, BLK)
            picked_ref[0, pl.ds(row, BLK), :] = ref[pl.ds(start, BLK), :]


def mixed_heads(result, gates, first):
    lane = lanes_of((BLK, 128))
    halves = []
    for pair in range(2):
        gated = []
        for head in (2 * pair, 2 * pair + 1):
            gate = gates[:, first + head : first + head + 1]
            gated.append(result[head * BLK : (head + 1) * BLK] * gate)
        halves.append(jnp.where(lane < HD, pltpu.roll(gated[0], HD, 1), gated[1]))
    return halves


def compressed_kernel(
    column0_ref, column1_ref, column2_ref, column3_ref, query_ref, gates_ref, outk_ref, outv_ref,
    turn_ref, mixed_ref, arrived_ref, key_ref, value_ref, score_ref, weight_ref,
):
    rank = kv_index()
    column = lax.axis_index("x")
    for d, ref in enumerate((column0_ref, column1_ref, column2_ref, column3_ref)):
        arrived_ref[(column - d + COLUMNS) % COLUMNS] = ref[...]
    flat = arrived_ref[...].reshape(PEERS * ROWS, 128)
    shape = (4 * PEERS, PEERS * ROWS)
    row = rows_of(shape)
    kind = row // PEERS
    source = row % PEERS + kind % 2
    target = (source % COLUMNS * LAYERS + source // COLUMNS) * ROWS + NSUM + jnp.where(kind == 0, 0, jnp.where(kind == 1, 2, jnp.where(kind == 2, 1, 3)))
    edges = dot(((lanes_of(shape) == target) & (source < PEERS)).astype(bf16), flat)
    pre_k = edges[:PEERS] + edges[PEERS : 2 * PEERS]
    pre_v = edges[2 * PEERS : 3 * PEERS] + edges[3 * PEERS :]
    ends = rows_of((PEERS, 128)) * TOK + TOK + CMP_STRIDE - 1
    last = squeeze_out(pre_k, pre_v, outk_ref[...], outv_ref[...], *turns(ends, turn_ref))
    is_last = rows_of((NSUM, 128)) == NSUM - 1
    lane = lanes_of((NSUM, 128))
    for peer in range(PEERS):
        chunk = arrived_ref[peer % COLUMNS, peer // COLUMNS, :NSUM, :].astype(f32)
        chunk = jnp.where(is_last, last[peer : peer + 1], chunk)
        value_ref[peer * NSUM : (peer + 1) * NSUM, :] = jnp.where(lane < HD, 1.0, chunk).astype(bf16)
        key_ref[peer * NSUM : (peer + 1) * NSUM, :] = chunk.astype(bf16)
    group = COMPRESSED * HEADS * BLK
    columns = lanes_of((HEADS * BLK, PEERS * NSUM))
    inside = lax.broadcasted_iota(jnp.int32, (HEADS * BLK, 1), 0) % BLK

    def score(step, carry):
        rows = query_ref[pl.ds(step * COMPRESSED, COMPRESSED)].reshape(group, 128)
        score_ref[pl.ds(pl.multiple_of(step * group, group), group), :] = dot_t(rows, key_ref[...])
        return carry

    def weigh(step, carry):
        for j in range(COMPRESSED):
            b = step * COMPRESSED + j
            rows = pl.ds(pl.multiple_of(b * HEADS * BLK, HEADS * BLK), HEADS * BLK)
            limit = (rank * TOK + b * BLK + inside - (2 * CMP_STRIDE - 1)) >> 4
            scores = jnp.where(columns <= limit, score_ref[rows, :], NEG)
            largest = jnp.maximum(jnp.max(scores, 1, keepdims=True), FLOOR)
            weight_ref[rows, :] = jnp.exp(scores - largest).astype(bf16)
        return carry

    def mix(step, carry):
        rows = pl.ds(pl.multiple_of(step * group, group), group)
        result = dot(weight_ref[rows, :], value_ref[...])
        result = result / jnp.maximum(pltpu.roll(result, HD, 1), 1.0)
        for j in range(COMPRESSED):
            start = pl.multiple_of((step * COMPRESSED + j) * BLK, BLK)
            one = result[j * HEADS * BLK : (j + 1) * HEADS * BLK]
            halves = mixed_heads(one, gates_ref[pl.ds(start, BLK), :], 0)
            mixed_ref[pl.ds(start, BLK), :128] = halves[0].astype(bf16)
            mixed_ref[pl.ds(start, BLK), 128:] = halves[1].astype(bf16)
        return carry

    lax.fori_loop(0, QB // COMPRESSED, score, 0)
    lax.fori_loop(0, QB // COMPRESSED, weigh, 0)
    lax.fori_loop(0, QB // COMPRESSED, mix, 0)


def selected_kernel(
    place_hbm, fetched_hbm, pair_hbm, query_hbm, bound_hbm, gates_hbm, mixed_hbm,
    out0_ref, out1_ref, out2_ref, out3_ref,
    place_ref, fetched_ref, pair_ref, query_ref, bound_ref, gates_ref, mixed_ref,
    key_ref, score_ref, weight_ref, out_ref, sems,
):
    chip = lax.axis_index("tp") // 2
    copies = [
        (place_hbm, place_ref),
        (fetched_hbm, fetched_ref),
        (pair_hbm.at[pl.ds(0, TOK)], pair_ref),
        (query_hbm, query_ref),
        (bound_hbm, bound_ref),
        (gates_hbm, gates_ref),
        (mixed_hbm, mixed_ref),
    ]
    copies = [pltpu.make_async_copy(a, b, sems.at[n]) for n, (a, b) in enumerate(copies)]
    for copy in copies:
        copy.start()
    inside = (lax.broadcasted_iota(jnp.int32, (HEADS * BLK, 1), 0) % BLK).astype(f32)
    lane = lanes_of((NSEL * BLK, 128))

    def score(step, carry):
        for j in range(GATHERED):
            b = step * GATHERED + j
            for k in range(NSEL):
                place = place_ref[b, k]
                far_row = pl.multiple_of(jnp.minimum(place, PEERS * CAP - 1) * BLK, BLK)
                near_row = pl.multiple_of(jnp.maximum(place - PEERS * CAP, 0) * BLK, BLK)
                is_near = jnp.full((BLK, 128), place, jnp.int32) >= PEERS * CAP
                key_ref[b, k * BLK : (k + 1) * BLK, :] = jnp.where(
                    is_near, pair_ref[pl.ds(near_row, BLK), :], fetched_ref[pl.ds(far_row, BLK), :]
                )
            score_ref[b] = dot_t(query_ref[b], key_ref[b])
        return carry

    def weigh(step, carry):
        for j in range(WEIGHED):
            b = step * WEIGHED + j
            scores = jnp.where(bound_ref[pl.ds(b, 1), :] <= inside, score_ref[b], NEG)
            largest = jnp.max(scores, 1, keepdims=True)
            weight_ref[b] = jnp.exp(scores - largest).astype(bf16)
        return carry

    def mix(step, carry):
        for j in range(MIXED):
            b = step * MIXED + j
            keys = key_ref[b]
            values = jnp.where(lane < HD, jnp.ones_like(keys), keys)
            result = dot(weight_ref[b], values)
            result = result / pltpu.roll(result, HD, 1)
            start = pl.multiple_of(b * BLK, BLK)
            halves = mixed_heads(result, gates_ref[pl.ds(start, BLK), :], HEADS)
            row = pl.multiple_of((b % PER_CHIP) * BLK, BLK)
            for side in range(2):
                cols = slice(128 * side, 128 * side + 128)
                out_ref[(b // PER_CHIP - chip + CHIPS) % CHIPS, pl.ds(row, BLK), cols] = (
                    mixed_ref[pl.ds(start, BLK), cols] + halves[side]
                ).astype(bf16)
        return carry

    for copy in copies[:4]:
        copy.wait()
    lax.fori_loop(0, QB // GATHERED, score, 0)
    copies[4].wait()
    lax.fori_loop(0, QB // WEIGHED, weigh, 0)
    copies[5].wait()
    copies[6].wait()
    lax.fori_loop(0, QB // MIXED, mix, 0)
    for d, ref in enumerate((out0_ref, out1_ref, out2_ref, out3_ref)):
        ref[...] = out_ref[d]


def output_kernel(
    a0_ref, a1_ref, a2_ref, a3_ref, w0_ref, w1_ref, w2_ref, w3_ref,
    mine_ref, other_ref, sum_ref,
):
    core = lax.axis_index("tp") % 2
    total = dot(a0_ref[...], w0_ref[...])
    total = total + dot(a1_ref[...], w1_ref[...])
    total = total + dot(a3_ref[...], w3_ref[...])
    total = total + dot(a2_ref[...], w2_ref[...])
    sum_ref[...] = total
    mine_ref[...] = sum_ref[pl.ds(pl.multiple_of(core * OUT_ROWS, OUT_ROWS), OUT_ROWS), :]
    other = pl.multiple_of((1 - core) * OUT_ROWS, OUT_ROWS)
    other_ref[...] = sum_ref[pl.ds(other, OUT_ROWS), :].astype(bf16)


VMEM = pl.BlockSpec(memory_space=pltpu.VMEM)
SMEM = pl.BlockSpec(memory_space=pltpu.SMEM)
HBM = pl.BlockSpec(memory_space=pltpu.HBM)


def shape_of(shape, dtype):
    return jax.ShapeDtypeStruct(shape, dtype)


def stored(shape, dtype):
    return pltpu.HBM(shape, dtype)


def far(*values):
    return [pltpu.with_memory_space_constraint(value, pltpu.HBM) for value in values]


def limit(mib):
    return pltpu.CompilerParams(vmem_limit_bytes=mib * 1024 * 1024)


def across(value, distance):
    return lax.ppermute(value, "z", [(i, (i + distance) % LAYERS) for i in range(LAYERS)])


def along(value, distance):
    return lax.ppermute(value, "x", [(i, (i + distance) % COLUMNS) for i in range(COLUMNS)])


def around(value, distance):
    route = [(2 * y + c, 2 * ((y + distance) % CHIPS) + c) for y in range(CHIPS) for c in range(2)]
    return lax.ppermute(value, "tp", route)


def on_device(
    tokens, query_weight, chosen_key_weight, chosen_value_weight, summary_key_weight,
    summary_value_weight, squeeze_key_in, squeeze_key_out, squeeze_value_in, squeeze_value_out,
    gate_weight, output_weight, chosen_blocks,
):
    chosen = chosen_blocks[0]
    squeeze_key_t = squeeze_key_out.T
    squeeze_value_t = squeeze_value_out.T
    turn = jnp.asarray(np.concatenate([INVERSE_ROW, SIGN_ROW], 0))
    payload, code, cosine, sine, place, bound = pl.pallas_call(
        token_kernel,
        name="tokens",
        out_shape=(
            stored((TOK + ROWS, 128), bf16),
            stored((8, NBLK), f32),
            stored((TOK, 128), f32),
            stored((TOK, 128), f32),
            stored((QB, NSEL), jnp.int32),
            stored((QB, NSEL * BLK), f32),
        ),
        in_specs=[HBM] * 11,
        out_specs=(VMEM,) * 6,
        scratch_shapes=[
            pltpu.VMEM((TOK, 2048), bf16),
            pltpu.VMEM((4 * HD, 2048), bf16),
            pltpu.VMEM((2048, 128), bf16),
            pltpu.VMEM((2048, 128), bf16),
            pltpu.VMEM((HD, 128), bf16),
            pltpu.VMEM((HD, 128), bf16),
            pltpu.VMEM((2, 128), f32),
            pltpu.VMEM((QB, NSEL), jnp.int32),
            pltpu.VMEM((TOK, 128), f32),
            pltpu.VMEM((2, TOK // 8, 128), f32),
            pltpu.SemaphoreType.DMA((10 + CHUNKS,)),
        ],
        compiler_params=limit(24),
        cost_estimate=pl.CostEstimate(flops=10**9, bytes_accessed=5 * 10**6, transcendentals=0),
    )(
        *far(
            tokens, summary_key_weight.T, summary_value_weight.T, chosen_key_weight.T,
            chosen_value_weight.T, squeeze_key_in, squeeze_value_in, squeeze_key_t, squeeze_value_t,
            turn, chosen,
        ),
    )
    up2 = across(payload, 2)
    down2 = across(payload, -2)
    up1 = across(payload, 1)
    down1 = across(payload, -1)
    codes = [code] + [along(code, d) for d in range(1, COLUMNS)]
    weight_1 = around(output_weight, 1)
    weight_3 = around(output_weight, -1)
    far_a = across(up2[:SPLIT], 2)
    far_b = across(down2[SPLIT:], -2)
    up3 = across(up2, 1)
    down3 = across(down2, -1)
    queries, gates, ids = pl.pallas_call(
        query_kernel,
        name="queries",
        out_shape=(
            stored((QB, HEADS * BLK, 128), bf16),
            stored((TOK, 2 * HEADS), f32),
            stored((PEERS, 128), jnp.int32),
        ),
        in_specs=[VMEM] * 9,
        out_specs=(VMEM,) * 3,
        scratch_shapes=[pltpu.VMEM((COLUMNS, 8, NBLK), f32)],
        compiler_params=limit(16),
        cost_estimate=pl.CostEstimate(flops=10**10, bytes_accessed=3 * 10**6, transcendentals=0),
    )(
        *far(tokens, query_weight), gate_weight.transpose(0, 2, 1), *far(cosine, sine, code), *codes[1:]
    )
    picked, column = pl.pallas_call(
        pick_kernel,
        name="pick",
        out_shape=(
            stored((COLUMNS, LAYERS * CAP * BLK, 128), bf16),
            stored((LAYERS, ROWS, 128), bf16),
        ),
        grid=(COLUMNS,),
        in_specs=[HBM] * 2 + [VMEM] * 8,
        out_specs=(pl.BlockSpec((1, LAYERS * CAP * BLK, 128), lambda n: (n, 0, 0)), VMEM),
        scratch_shapes=[
            pltpu.VMEM((TOK + ROWS, 128), bf16),
            pltpu.VMEM((TOK + ROWS, 128), bf16),
            pltpu.SMEM((PEERS, 128), jnp.int32),
            pltpu.SemaphoreType.DMA((2,)),
        ],
        compiler_params=limit(8),
    )(*far(ids, payload), up1, up2, up3, far_a, far_b, down3, down2, down1)
    fetched = lax.all_to_all(picked, "x", 0, 0, tiled=True)
    columns = [column] + [along(column, d) for d in range(1, COLUMNS)]
    weight_2 = around(weight_1, 1)
    mixed = pl.pallas_call(
        compressed_kernel,
        name="compressed",
        out_shape=stored((TOK, HEADS * HD), bf16),
        in_specs=[VMEM] * (COLUMNS + 5),
        out_specs=VMEM,
        scratch_shapes=[
            pltpu.VMEM((COLUMNS, LAYERS, ROWS, 128), bf16),
            pltpu.VMEM((PEERS * NSUM, 128), bf16),
            pltpu.VMEM((PEERS * NSUM, 128), bf16),
            pltpu.VMEM((QB * HEADS * BLK, PEERS * NSUM), f32),
            pltpu.VMEM((QB * HEADS * BLK, PEERS * NSUM), bf16),
        ],
        compiler_params=limit(24),
        cost_estimate=pl.CostEstimate(flops=10**10, bytes_accessed=3 * 10**6, transcendentals=0),
    )(*columns, *far(queries, gates, squeeze_key_t, squeeze_value_t, turn))
    pieces = pl.pallas_call(
        selected_kernel,
        name="selected",
        out_shape=(shape_of((PER_CHIP * BLK, HEADS * HD), bf16),) * CHIPS,
        in_specs=[HBM] * 7,
        out_specs=(VMEM,) * CHIPS,
        scratch_shapes=[
            pltpu.SMEM((QB, NSEL), jnp.int32),
            pltpu.VMEM((PEERS * CAP * BLK, 128), bf16),
            pltpu.VMEM((TOK, 128), bf16),
            pltpu.VMEM((QB, HEADS * BLK, 128), bf16),
            pltpu.VMEM((QB, NSEL * BLK), f32),
            pltpu.VMEM((TOK, 2 * HEADS), f32),
            pltpu.VMEM((TOK, HEADS * HD), bf16),
            pltpu.VMEM((QB, NSEL * BLK, 128), bf16),
            pltpu.VMEM((QB, HEADS * BLK, NSEL * BLK), f32),
            pltpu.VMEM((QB, HEADS * BLK, NSEL * BLK), bf16),
            pltpu.VMEM((CHIPS, PER_CHIP * BLK, HEADS * HD), bf16),
            pltpu.SemaphoreType.DMA((7,)),
        ],
        compiler_params=limit(24),
        cost_estimate=pl.CostEstimate(flops=10**9, bytes_accessed=3 * 10**6, transcendentals=0),
    )(
        *far(place, fetched.reshape(PEERS * CAP * BLK, 128), payload, queries, bound, gates, mixed),
    )
    piece_2 = around(pieces[2], 2)
    piece_1 = around(pieces[1], 1)
    piece_3 = around(pieces[3], -1)
    mine, other = pl.pallas_call(
        output_kernel,
        name="output",
        out_shape=(shape_of((OUT_ROWS, 2048), f32), shape_of((OUT_ROWS, 2048), bf16)),
        in_specs=[VMEM] * 8,
        out_specs=(VMEM, VMEM),
        scratch_shapes=[pltpu.VMEM((2 * OUT_ROWS, 2048), f32)],
        compiler_params=limit(16),
    )(
        pieces[0], piece_1, piece_2, piece_3, output_weight, weight_1, weight_2, weight_3,
    )
    swapped = lax.ppermute(other, "tp", [(i, i ^ 1) for i in range(2 * CHIPS)])
    return (mine + swapped.astype(f32)).astype(bf16)


def solution(mesh):
    split = Mesh(mesh.devices.reshape(LAYERS, COLUMNS, 2 * CHIPS), ("z", "x", "tp"))
    kv = ("z", "x")
    return jax.shard_map(
        on_device,
        mesh=split,
        in_specs=(
            P(kv, None),
            P(None, "tp"),
            P(None, "tp"),
            P(None, "tp"),
            P(None, "tp"),
            P(None, "tp"),
            P(),
            P(),
            P(),
            P(),
            P(None, None, "tp"),
            P("tp", None),
            P("tp", kv, None),
        ),
        out_specs=P(("z", "x", "tp"), None),
        check_vma=False,
    )
```
